32 devices in a mesh: kv: 16 (over z, y, x), tp: 2 (over core).
Axes of the slice: x: 2, y: 2, z: 4, core: 2. Of those that a mesh axis runs over, the one named last changes fastest.
Arguments:
- tokens: bfloat16 [6144, 2048], P('kv', 'tp'), may hold values from -12 to 12
- query_weight: bfloat16 [2048, 2048], P(None, 'tp'), may hold values from -0.5 to 0.5
- key_weight: bfloat16 [2048, 1024], P(None, 'tp'), may hold values from -0.5 to 0.5
- value_weight: bfloat16 [2048, 1024], P(None, 'tp'), may hold values from -0.125 to 0.125
- out_weight: bfloat16 [2048, 2048], P(None, 'tp'), may hold values from -0.125 to 0.125
- chosen: int32 [96, 16], P('kv'), may hold values from 0 to 95, as said below
Outputs:
- mixed: bfloat16 [6144, 2048], P('kv', 'tp')
The draws below stay inside these ranges and needn't reach their ends.
Inputs may be any that keep to these rules, and one draw needn't show every extreme that they name: `chosen`: row b names no block after b; its first entry is b and its next 3 entries are blocks of the same device as block b; entries may repeat. Over the rows of one device, the entries after the first 4 name at most 2 blocks, counting repeats, of any one other device, and some device names exactly 2 of another.
All inputs are finite; a program needn't handle non-finite values.
Results may differ from the reference program's by a relative error of at most 0.0072.
Values may be sent and summed in bfloat16 or wider, within the bound.
No kernel may reach another device: no remote copies, remote signals or barrier semaphores. Data moves between devices by JAX's collectives and lax.ppermute only.
A program may use at most 128 MiB of HBM per device.

```python
import jax
import jax.numpy as jnp
from jax import lax

D = 2048
H = 16
KVH = 8
HD = 128
BLK = 64
TOPB = 16
LOCAL = 3
CAP = 2
TOK_DEV = 384
TOKENS = 6144
NQB = 96
N_KV = 16


def draw_tokens(key, part):
    plain = jnp.clip(jax.random.normal(key, (TOKENS, D), jnp.float32), -6.0, 6.0)
    return plain.astype(jnp.bfloat16)


def draw_query_weight(key, part):
    fresh = jax.random.normal(jax.random.fold_in(key, 11), (D, H * HD), jnp.float32)
    return jnp.clip(fresh * D ** (-0.5), -0.5, 0.5).astype(jnp.bfloat16)


def draw_key_weight(key, part):
    fresh = jax.random.normal(jax.random.fold_in(key, 12), (D, KVH * HD), jnp.float32)
    return jnp.clip(fresh * D ** (-0.5), -0.5, 0.5).astype(jnp.bfloat16)


def draw_chosen(key, part):
    blocks = TOK_DEV // BLK
    far_count = TOPB - 1 - LOCAL
    ask_count = blocks * far_count
    picked = min(ask_count // CAP, N_KV)
    streams = jax.random.split(jax.random.fold_in(key, 21), 6)
    devices = jnp.arange(N_KV, dtype=jnp.int32)
    asking = devices[:, None]
    target = devices[None, :]
    raw_score = jax.random.randint(streams[0], (N_KV, N_KV), 0, 1 << 14)
    popular = jax.random.randint(streams[1], (1, N_KV), 0, 4) == 0
    forced = (target == asking - 1) | (target == asking - N_KV // 2)
    scores = raw_score * 1024 + target
    scores = scores + jnp.where(popular, 1 << 25, 0) + jnp.where(forced, 1 << 26, 0)
    scores = jnp.where(target < asking, scores, -1 - target)
    ranked = lax.top_k(scores, picked)[1].astype(jnp.int32)
    usable = jnp.minimum(devices, picked)
    request = jnp.arange(ask_count, dtype=jnp.int32)
    owner_slot = request // CAP
    holder = jnp.take_along_axis(ranked, jnp.broadcast_to(jnp.minimum(owner_slot, picked - 1)[None, :], (N_KV, ask_count)), axis=1)
    usable_slot = owner_slot[None, :] < usable[:, None]
    hot_block = jax.random.randint(streams[2], (N_KV,), 0, blocks)
    coin_flip = jax.random.randint(streams[3], (N_KV, ask_count), 0, 2)
    any_block = jax.random.randint(streams[4], (N_KV, ask_count), 0, blocks)
    inside = jnp.where(coin_flip == 0, hot_block[holder], any_block)
    query_block = devices[:, None] * blocks + request[None, :] // far_count
    far_ids = jnp.where(usable_slot, holder * blocks + inside, query_block).reshape(N_KV, blocks, far_count)
    own_ids = devices[:, None] * blocks + jnp.arange(blocks, dtype=jnp.int32)[None, :]
    near_raw = jax.random.randint(streams[5], (N_KV, blocks, LOCAL), 0, 1 << 16)
    near_ids = devices[:, None, None] * blocks + near_raw % (jnp.arange(blocks, dtype=jnp.int32)[None, :, None] + 1)
    table_rows = jnp.concatenate([own_ids[:, :, None], near_ids, far_ids], axis=2)
    return table_rows.reshape(N_KV * blocks, TOPB).astype(jnp.int32)


def steps_of(rng, extent, cuts, low, largest):
    loudness = 1.0
    for axis_at, blocks in cuts:
        steps = jax.random.uniform(jax.random.fold_in(jax.random.fold_in(rng, 6), axis_at), (blocks,), jnp.float32, low / len(cuts), largest / len(cuts))
        loudness = loudness * jnp.repeat(jnp.exp(steps), extent[axis_at] // blocks).reshape((-1,) + (1,) * (len(extent) - 1 - axis_at))
    return loudness


def centred(rng, dims, width, limit, cuts=(), kind=jnp.bfloat16):
    values = jax.random.normal(rng, dims, jnp.float32) * width
    if len(cuts) > 0:
        values = steps_of(rng, dims, cuts, -0.22, 0.18) * values
    return jnp.clip(values, min=-limit, max=limit).astype(kind)


def setup_inputs(seed: int = 0) -> dict:
    keys = jax.random.split(jax.random.key(seed), 7)
    return {
        "tokens": draw_tokens(jax.random.fold_in(keys[6], 71), 0),
        "query_weight": draw_query_weight(jax.random.fold_in(keys[6], 71), 0),
        "key_weight": draw_key_weight(jax.random.fold_in(keys[6], 71), 0),
        "value_weight": centred(keys[3], (D, KVH * HD), D ** -0.5, 0.125, ((1, 2),)),
        "out_weight": centred(keys[4], (H * HD, D), (H * HD) ** -0.5, 0.125, ((1, 2),)),
        "chosen": draw_chosen(jax.random.fold_in(keys[6], 71), 0),
    }


def reference(tokens, query_weight, key_weight, value_weight, out_weight, chosen):
    queries = jnp.dot(tokens, query_weight, preferred_element_type=jnp.float32).astype(jnp.bfloat16)
    key_rows = jnp.dot(tokens, key_weight, preferred_element_type=jnp.float32).astype(jnp.bfloat16)
    value_rows = jnp.dot(tokens, value_weight, preferred_element_type=jnp.float32).astype(jnp.bfloat16)
    group_size = H // KVH
    grouped = queries.reshape(NQB, BLK, KVH, group_size, HD)
    key_blocks = key_rows.reshape(NQB, BLK, KVH, HD)
    value_blocks = value_rows.reshape(NQB, BLK, KVH, HD)

    def attend(inputs):
        block_queries, chosen_row, block_number = inputs
        slot_order = jnp.arange(TOPB)
        repeats = jnp.any((chosen_row[:, None] == chosen_row[None, :]) & (slot_order[None, :] < slot_order[:, None]), axis=1)
        got_keys = jnp.take(key_blocks, chosen_row, axis=0).reshape(TOPB * BLK, KVH, HD)
        got_values = jnp.take(value_blocks, chosen_row, axis=0).reshape(TOPB * BLK, KVH, HD)
        scores = jnp.einsum("qkgd,skd->kgqs", block_queries.astype(jnp.float32), got_keys.astype(jnp.float32),
                            precision=lax.Precision.HIGHEST) * (HD ** -0.5)
        query_pos = block_number * BLK + jnp.arange(BLK, dtype=jnp.int32)
        key_pos = (chosen_row[:, None] * BLK + jnp.arange(BLK, dtype=jnp.int32)[None, :]).reshape(-1)
        fresh_slot = jnp.broadcast_to((~repeats)[:, None], (TOPB, BLK)).reshape(-1)
        visible = fresh_slot[None, :] & (key_pos[None, :] <= query_pos[:, None])
        scores = jnp.where(visible[None, None], scores, -jnp.inf)
        row_peak = jnp.max(scores, axis=-1, keepdims=True)
        weights = jnp.exp(scores - row_peak)
        row_total = jnp.sum(weights, axis=-1)
        rounded = lax.optimization_barrier(weights.astype(jnp.bfloat16)).astype(jnp.float32)
        mixed_heads = jnp.einsum("kgqs,skd->qkgd", rounded, got_values.astype(jnp.float32),
                                 precision=lax.Precision.HIGHEST)
        mixed_heads = mixed_heads / jnp.transpose(row_total, (2, 0, 1))[..., None]
        return mixed_heads.astype(jnp.bfloat16).reshape(BLK, H * HD)

    heads_out = lax.map(attend, (grouped, chosen, jnp.arange(NQB, dtype=jnp.int32)))
    return jnp.dot(heads_out.reshape(TOKENS, H * HD), out_weight, preferred_element_type=jnp.float32).astype(jnp.bfloat16)
```

```python
import functools

import jax
import jax.numpy as jnp
from jax import lax
from jax.experimental import pallas as pl
from jax.experimental.pallas import tpu as pltpu
from jax.sharding import PartitionSpec as P

HD = 128
BLK = 64
TOPB = 16
CAP = 2
NEG = float("-inf")


def spread(part):
    count = lax.axis_size("tp")
    pieces = [part]
    for shift in range(1, count):
        pairs = [(i, (i - shift) % count) for i in range(count)]
        pieces.append(lax.ppermute(part, "tp", pairs))
    return pieces


def split_dot(pieces, weight):
    count = lax.axis_size("tp")
    me = lax.axis_index("tp")
    width = weight.shape[0] // count
    total = None
    for shift, piece in enumerate(pieces):
        rows = lax.dynamic_slice_in_dim(weight, (me + shift) % count * width, width, 0)
        term = jnp.dot(piece, rows, preferred_element_type=jnp.float32)
        total = term if total is None else total + term
    return total.astype(jnp.bfloat16)


def attend_kernel(sizes, heads, group, *refs):
    n = len(sizes)
    slots_ref, bias_ref, q_ref = refs[:3]
    pool_refs = refs[3 : 3 + n]
    out_ref, pool, sems = refs[3 + n :]
    width = heads * HD
    copies = []
    at = 0
    for i, size in enumerate(sizes):
        copies.append(
            pltpu.make_async_copy(pool_refs[i], pool.at[pl.ds(at, size)], sems.at[i])
        )
        at += size
    for copy in copies:
        copy.start()
    for copy in copies:
        copy.wait()
    span = TOPB * BLK
    rows = group * BLK
    tri_row = lax.broadcasted_iota(jnp.int32, (BLK, HD), 0)
    tri_col = lax.broadcasted_iota(jnp.int32, (BLK, HD), 1)
    tri = jnp.where((tri_col < BLK) & (tri_col > tri_row), NEG, 0.0)
    tri = jnp.concatenate([tri] * group, axis=0)

    def block(b, carry):
        at_row = pl.multiple_of(b * BLK, BLK)
        bias = bias_ref[pl.ds(b, 1)].reshape(1, span)
        picks = [slots_ref[b * TOPB + s] for s in range(TOPB)]
        for j in range(heads):
            cols = [(j * group + g) * HD for g in range(group)]
            q = jnp.concatenate(
                [q_ref[pl.ds(at_row, BLK), c : c + HD] for c in cols], axis=0
            )
            k = jnp.concatenate(
                [pool[p, :, j * HD : (j + 1) * HD] for p in picks], axis=0
            )
            v = jnp.concatenate(
                [pool[p, :, width + j * HD : width + (j + 1) * HD] for p in picks], axis=0
            )
            s = lax.dot_general(
                q, k, (((1,), (1,)), ((), ())), preferred_element_type=jnp.float32
            )
            s = s + bias
            s = jnp.concatenate([s[:, :HD] + tri, s[:, HD:]], axis=1)
            peak = jnp.max(s, axis=1, keepdims=True)
            w = jnp.exp((s - peak) * HD ** (-0.5))
            total = jnp.sum(w, axis=1, keepdims=True)
            o = jnp.dot(w.astype(jnp.bfloat16), v, preferred_element_type=jnp.float32)
            o = (o / total).astype(jnp.bfloat16)
            for g, c in enumerate(cols):
                out_ref[pl.ds(at_row, BLK), c : c + HD] = o[g * BLK : (g + 1) * BLK]
        return carry

    lax.fori_loop(0, q_ref.shape[0] // BLK, block, 0)


def attend(queries, slots, bias, pools, heads):
    rows, cols = queries.shape
    group = cols // HD // heads
    sizes = tuple(p.shape[0] for p in pools)
    vmem = pl.BlockSpec(memory_space=pltpu.VMEM)
    return pl.pallas_call(
        functools.partial(attend_kernel, sizes, heads, group),
        out_shape=jax.ShapeDtypeStruct((rows, cols), jnp.bfloat16),
        in_specs=[pl.BlockSpec(memory_space=pltpu.SMEM), vmem, vmem]
        + [pl.BlockSpec(memory_space=pl.ANY)] * len(pools),
        out_specs=vmem,
        scratch_shapes=[
            pltpu.VMEM((sum(sizes), BLK, 2 * heads * HD), jnp.bfloat16),
            pltpu.SemaphoreType.DMA((len(sizes),)),
        ],
        cost_estimate=pl.CostEstimate(
            flops=4 * rows * TOPB * BLK * cols,
            bytes_accessed=4 * rows * cols + 4 * sum(sizes) * BLK * heads * HD,
            transcendentals=rows * TOPB * BLK * cols // HD,
        ),
        name="attend",
    )(slots, bias, queries, *pools)


def local(tokens, query_weight, key_weight, value_weight, out_weight, chosen):
    tok_rows = tokens.shape[0]
    key_cols = key_weight.shape[1]
    key_heads = key_cols // HD
    own_blocks = tok_rows // BLK
    device = lax.axis_index("kv")
    key_devices = lax.axis_size("kv")
    section = spread(tokens)
    keys = split_dot(section, key_weight)
    values = split_dot(section, value_weight)
    own_pairs = jnp.concatenate([keys, values], axis=1).reshape(own_blocks, BLK, 2 * key_cols)
    wanted = chosen.reshape(-1)
    holder = wanted // own_blocks
    within = wanted % own_blocks
    remote = holder != device
    slot_index = jnp.arange(wanted.shape[0])
    earlier = (
        (slot_index[None, :] < slot_index[:, None])
        & (holder[None, :] == holder[:, None])
        & remote[None, :]
    )
    places = jnp.sum(earlier.astype(jnp.int32), axis=1)
    owner_ids = jnp.arange(key_devices)[:, None, None]
    place_ids = jnp.arange(CAP)[None, :, None]
    matches = (
        remote[None, None, :]
        & (holder[None, None, :] == owner_ids)
        & (places[None, None, :] == place_ids)
    )
    request_table = jnp.sum(jnp.where(matches, within[None, None, :], 0), axis=2)
    incoming = lax.all_to_all(request_table, "kv", split_axis=0, concat_axis=0, tiled=True)
    outgoing = jnp.take(own_pairs, incoming.reshape(-1), axis=0).reshape(
        key_devices, CAP, BLK, 2 * key_cols
    )
    arrived = lax.all_to_all(outgoing, "kv", split_axis=0, concat_axis=0, tiled=True)
    arrived = arrived.reshape(key_devices * CAP, BLK, 2 * key_cols)
    queries = split_dot(section, query_weight)
    far = own_blocks + holder * CAP + jnp.minimum(places, CAP - 1)
    slots = jnp.where(remote, far, within).astype(jnp.int32)
    slot_order = jnp.arange(TOPB)
    repeats = jnp.any(
        (chosen[:, :, None] == chosen[:, None, :])
        & (slot_order[None, None, :] < slot_order[None, :, None]),
        axis=2,
    )
    bias = jnp.where(repeats, NEG, 0.0).astype(jnp.float32)
    bias = jnp.broadcast_to(bias[:, :, None], (own_blocks, TOPB, BLK)).reshape(own_blocks, -1)
    heads_out = attend(queries, slots, bias, [own_pairs, arrived], key_heads)
    return split_dot(spread(heads_out), out_weight)


def solution(mesh):
    return jax.shard_map(
        local,
        mesh=mesh,
        in_specs=(
            P("kv", "tp"),
            P(None, "tp"),
            P(None, "tp"),
            P(None, "tp"),
            P(None, "tp"),
            P("kv", None),
        ),
        out_specs=P("kv", "tp"),
        check_vma=False,
    )
```

```python
import functools
import math

import jax
import jax.numpy as jnp
from jax import lax
from jax.experimental import pallas as pl
from jax.experimental.pallas import tpu as pltpu
from jax.sharding import PartitionSpec as P

HD = 128
BLK = 64
TOPB = 16
CAP = 2
NEG = float("-inf")
VMEM = pl.BlockSpec(memory_space=pltpu.VMEM)
SMEM = pl.BlockSpec(memory_space=pltpu.SMEM)
ANY = pl.BlockSpec(memory_space=pl.ANY)


def plane_size(devices):
    return max(d for d in range(1, math.isqrt(devices) + 1) if devices % d == 0)


def partner(place, shift, plane):
    if plane & (plane - 1) == 0:
        return place ^ shift
    return (shift - place) % plane


def spread(part):
    count = lax.axis_size("tp")
    pieces = [part]
    for shift in range(1, count):
        pairs = [(i, (i - shift) % count) for i in range(count)]
        pieces.append(lax.ppermute(part, "tp", pairs))
    return pieces


def split_dot(pieces, weight):
    count = lax.axis_size("tp")
    me = lax.axis_index("tp")
    width = weight.shape[0] // count
    total = None
    for shift, piece in enumerate(pieces):
        rows = lax.dynamic_slice_in_dim(weight, (me + shift) % count * width, width, 0)
        term = jnp.dot(piece, rows, preferred_element_type=jnp.float32)
        total = term if total is None else total + term
    return total.astype(jnp.bfloat16)


def project_kernel(count, first, cols, *refs):
    starts_ref = refs[0]
    pieces = refs[1 : 1 + count]
    key_ref, value_ref, out_ref, held, sems = refs[1 + count :]
    width = pieces[0].shape[1]
    copies = []
    for s in range(count):
        at = pl.multiple_of(starts_ref[s], width)
        for i, ref in enumerate((key_ref, value_ref)):
            copy = pltpu.make_async_copy(
                ref.at[pl.ds(at, width), pl.ds(first, cols)],
                held.at[s, i],
                sems.at[s, i],
            )
            copy.start()
            copies.append(copy)
    totals = [None, None]
    for s in range(count):
        for i in range(2):
            copies[2 * s + i].wait()
            term = jnp.dot(
                pieces[s][...], held[s, i], preferred_element_type=jnp.float32
            )
            totals[i] = term if s == 0 else totals[i] + term
    for i in range(2):
        out_ref[:, i * cols : (i + 1) * cols] = totals[i].astype(jnp.bfloat16)


def project(pieces, starts, key_weight, value_weight, first, cols):
    rows, width = pieces[0].shape
    count = len(pieces)
    return pl.pallas_call(
        functools.partial(project_kernel, count, first, cols),
        out_shape=jax.ShapeDtypeStruct((rows, 2 * cols), jnp.bfloat16),
        in_specs=[SMEM] + [VMEM] * count + [ANY, ANY],
        out_specs=VMEM,
        scratch_shapes=[
            pltpu.VMEM((count, 2, width, cols), jnp.bfloat16),
            pltpu.SemaphoreType.DMA((count, 2)),
        ],
        cost_estimate=pl.CostEstimate(
            flops=4 * rows * width * count * cols,
            bytes_accessed=2 * count * width * (rows + 2 * cols) + 4 * rows * cols,
            transcendentals=0,
        ),
        name="project",
    )(starts, *pieces, key_weight, value_weight)


def attend_kernel(sizes, heads, group, first, *refs):
    n = len(sizes)
    slots_ref, bias_ref, q_ref = refs[:3]
    pool_refs = refs[3 : 3 + n]
    out_ref, pool, sems = refs[3 + n :]
    width = heads * HD
    copies = []
    at = 0
    for i, size in enumerate(sizes):
        copies.append(
            pltpu.make_async_copy(pool_refs[i], pool.at[pl.ds(at, size)], sems.at[i])
        )
        at += size
    for copy in copies:
        copy.start()
    for copy in copies:
        copy.wait()
    span = TOPB * BLK
    tri_row = lax.broadcasted_iota(jnp.int32, (BLK, HD), 0)
    tri_col = lax.broadcasted_iota(jnp.int32, (BLK, HD), 1)
    tri = jnp.where((tri_col < BLK) & (tri_col > tri_row), NEG, 0.0)
    tri = jnp.concatenate([tri] * group, axis=0)

    def block(b, carry):
        at_row = pl.multiple_of(b * BLK, BLK)
        bias = bias_ref[pl.ds(b, 1)].reshape(1, span)
        picks = [slots_ref[b * TOPB + s] for s in range(TOPB)]
        for j in range(heads):
            cols = [(j * group + g) * HD for g in range(group)]
            q = jnp.concatenate(
                [q_ref[pl.ds(at_row, BLK), first + c : first + c + HD] for c in cols],
                axis=0,
            )
            k = jnp.concatenate(
                [pool[p, :, j * HD : (j + 1) * HD] for p in picks], axis=0
            )
            v = jnp.concatenate(
                [pool[p, :, width + j * HD : width + (j + 1) * HD] for p in picks], axis=0
            )
            s = lax.dot_general(
                q, k, (((1,), (1,)), ((), ())), preferred_element_type=jnp.float32
            )
            s = s + bias
            s = jnp.concatenate([s[:, :HD] + tri, s[:, HD:]], axis=1)
            peak = jnp.max(s, axis=1, keepdims=True)
            w = jnp.exp((s - peak) * HD ** (-0.5))
            total = jnp.sum(w, axis=1, keepdims=True)
            o = jnp.dot(w.astype(jnp.bfloat16), v, preferred_element_type=jnp.float32)
            o = (o / total).astype(jnp.bfloat16)
            for g, c in enumerate(cols):
                out_ref[pl.ds(at_row, BLK), c : c + HD] = o[g * BLK : (g + 1) * BLK]
        return carry

    lax.fori_loop(0, q_ref.shape[0] // BLK, block, 0)


def attend(queries, slots, bias, pools, heads, group, first):
    rows = queries.shape[0]
    cols = heads * group * HD
    sizes = tuple(p.shape[0] for p in pools)
    return pl.pallas_call(
        functools.partial(attend_kernel, sizes, heads, group, first),
        out_shape=jax.ShapeDtypeStruct((rows, cols), jnp.bfloat16),
        in_specs=[SMEM, VMEM, VMEM] + [ANY] * len(pools),
        out_specs=VMEM,
        scratch_shapes=[
            pltpu.VMEM((sum(sizes), BLK, 2 * heads * HD), jnp.bfloat16),
            pltpu.SemaphoreType.DMA((len(sizes),)),
        ],
        cost_estimate=pl.CostEstimate(
            flops=4 * rows * TOPB * BLK * cols,
            bytes_accessed=4 * rows * cols + 4 * sum(sizes) * BLK * heads * HD,
            transcendentals=rows * TOPB * BLK * cols // HD,
        ),
        name="attend",
    )(slots, bias, queries, *pools)


def local(tokens, query_weight, key_weight, value_weight, out_weight, chosen):
    tok_rows = tokens.shape[0]
    key_heads = key_weight.shape[1] // HD
    group = query_weight.shape[1] // HD // key_heads
    own_blocks = tok_rows // BLK
    device = lax.axis_index("kv")
    devices = lax.axis_size("kv")
    plane = plane_size(devices)
    lines = devices // plane
    line = device // plane
    place = device % plane
    tp = lax.axis_size("tp")
    streams = 2 if key_heads % 2 == 0 else 1
    heads = key_heads // streams
    cols = heads * HD

    section = spread(tokens)
    width = tokens.shape[1]
    starts = (lax.axis_index("tp") + jnp.arange(tp, dtype=jnp.int32)) % tp * width

    wanted = chosen.reshape(-1)
    holder = wanted // own_blocks
    within = wanted - holder * own_blocks
    remote = holder != device
    slot_index = jnp.arange(wanted.shape[0])
    earlier = (
        (slot_index[None, :] < slot_index[:, None])
        & (holder[None, :] == holder[:, None])
        & remote[None, :]
    )
    places = jnp.sum(earlier.astype(jnp.int32), axis=1)
    matches = (
        remote[None, None, :]
        & (holder[None, None, :] == jnp.arange(devices)[:, None, None])
        & (places[None, None, :] == jnp.arange(CAP)[None, :, None])
    )
    requests = jnp.sum(jnp.where(matches, within[None, None, :], 0), axis=2)
    requests = requests.reshape(lines, plane, CAP)

    def swap(shift, low, forward_only):
        return [
            (l * plane + c, l * plane + partner(c, shift, plane))
            for l in range(low, lines)
            for c in range(plane)
            if partner(c, shift, plane) != c
            and (c < partner(c, shift, plane) or not forward_only)
        ]

    asked = []
    for shift in range(1, plane):
        mine = lax.dynamic_index_in_dim(
            requests, partner(place, shift, plane), 1, keepdims=False
        )
        asked.append(lax.ppermute(mine, "kv", swap(shift, 0, False)))
    asked = jnp.stack(asked, axis=0) if asked else None

    holder_line = holder // plane
    holder_place = holder - holder_line * plane
    gap = line - holder_line
    shift_to = jnp.bitwise_xor(holder_place, place)
    if plane & (plane - 1) != 0:
        shift_to = (holder_place + place) % plane
    same = holder_place == place
    line_at = own_blocks + (gap - 1) * own_blocks + within
    side_base = own_blocks * lines
    side_at = side_base + (gap * (plane - 1) + shift_to - 1) * CAP
    side_at = side_at + jnp.minimum(places, CAP - 1)
    slots = jnp.where(remote, jnp.where(same, line_at, side_at), within)
    slots = jnp.clip(slots, 0, side_base + lines * (plane - 1) * CAP - 1).astype(jnp.int32)

    slot_order = jnp.arange(TOPB)
    repeats = jnp.any(
        (chosen[:, :, None] == chosen[:, None, :])
        & (slot_order[None, None, :] < slot_order[None, :, None]),
        axis=2,
    )
    bias = jnp.where(repeats, NEG, 0.0).astype(jnp.float32)
    bias = jnp.broadcast_to(bias[:, :, None], (own_blocks, TOPB, BLK)).reshape(own_blocks, -1)

    up = {
        low: [(d, d + plane) for d in range(low * plane, devices - plane)]
        for low in range(lines)
    }
    held = []
    for t in range(streams):
        pair = project(section, starts, key_weight, value_weight, t * cols, cols)
        held.append(pair.reshape(own_blocks, BLK, 2 * cols))
    own = list(held)
    line_parts = [[] for _ in range(streams)]
    side_parts = [[] for _ in range(streams)]
    for step in range(lines):
        for t in range(streams):
            here = held[t]
            if step < lines - 1:
                held[t] = lax.ppermute(here, "kv", up[step])
                line_parts[t].append(held[t])
            for shift in range(1, plane):
                row = lax.dynamic_index_in_dim(
                    asked[shift - 1], jnp.maximum(line - step, 0), 0, keepdims=False
                )
                picked = [
                    lax.dynamic_slice_in_dim(here, row[i], 1, 0) for i in range(CAP)
                ]
                picked = jnp.concatenate(picked, axis=0)
                side_parts[t].append(
                    lax.ppermute(picked, "kv", swap(shift, step, step == 0))
                )
    queries = split_dot(section, query_weight)
    done = []
    for t in range(streams):
        pools = [own[t]] + line_parts[t] + side_parts[t]
        done.append(
            attend(queries, slots, bias, pools, heads, group, t * cols * group)
        )
    heads_out = jnp.concatenate(done, axis=1)
    return split_dot(spread(heads_out), out_weight)


def solution(mesh):
    return jax.shard_map(
        local,
        mesh=mesh,
        in_specs=(
            P("kv", "tp"),
            P(None, "tp"),
            P(None, "tp"),
            P(None, "tp"),
            P(None, "tp"),
            P("kv", None),
        ),
        out_specs=P("kv", "tp"),
        check_vma=False,
    )
```

```python
import functools
import math

import jax
import jax.numpy as jnp
from jax import lax
from jax.experimental import pallas as pl
from jax.experimental.pallas import tpu as pltpu
from jax.sharding import PartitionSpec as P


HD = 128
BLK = 64
TOPB = 16
CAP = 2
NEG = float("-inf")
VMEM = pl.BlockSpec(memory_space=pltpu.VMEM)
SMEM = pl.BlockSpec(memory_space=pltpu.SMEM)
ANY = pl.BlockSpec(memory_space=pl.ANY)


def plane_size(devices):
    return max(d for d in range(1, math.isqrt(devices) + 1) if devices % d == 0)


def partner(place, shift, plane):
    if plane & (plane - 1) == 0:
        return place ^ shift
    return (shift - place) % plane


def far(part):
    return pltpu.with_memory_space_constraint(part, pltpu.HBM)


def send(part, pairs):
    return lax.ppermute(part, "kv", pairs)


def spread(part):
    count = lax.axis_size("tp")
    pieces = [part]
    for shift in range(1, count):
        pairs = [(i, (i - shift) % count) for i in range(count)]
        pieces.append(lax.ppermute(part, "tp", pairs))
    return pieces


def split_dot(pieces, weight):
    count = lax.axis_size("tp")
    me = lax.axis_index("tp")
    width = weight.shape[0] // count
    total = None
    for shift, piece in enumerate(pieces):
        rows = lax.dynamic_slice_in_dim(weight, (me + shift) % count * width, width, 0)
        term = jnp.dot(piece, rows, preferred_element_type=jnp.float32)
        total = term if total is None else total + term
    return total.astype(jnp.bfloat16)


def project_kernel(count, first, cols, *refs):
    pieces = refs[:count]
    key_ref, value_ref, out_ref, held, sems = refs[count:]
    width = pieces[0].shape[1]
    me = lax.axis_index("tp")
    copies = []
    for s in range(count):
        at = pl.multiple_of(lax.rem(me + s, count) * width, width)
        for i, ref in enumerate((key_ref, value_ref)):
            copy = pltpu.make_async_copy(
                ref.at[pl.ds(at, width), pl.ds(first, cols)],
                held.at[s, i],
                sems.at[s, i],
            )
            copy.start()
            copies.append(copy)
    totals = [None, None]
    for s in range(count):
        for i in range(2):
            copies[2 * s + i].wait()
            term = jnp.dot(
                pieces[s][...], held[s, i], preferred_element_type=jnp.float32
            )
            totals[i] = term if s == 0 else totals[i] + term
    for i in range(2):
        out_ref[:, i * cols : (i + 1) * cols] = totals[i].astype(jnp.bfloat16)


def project(pieces, key_weight, value_weight, first, cols):
    rows, width = pieces[0].shape
    count = len(pieces)
    return pl.pallas_call(
        functools.partial(project_kernel, count, first, cols),
        out_shape=jax.ShapeDtypeStruct((rows, 2 * cols), jnp.bfloat16),
        in_specs=[VMEM] * count + [ANY, ANY],
        out_specs=VMEM,
        scratch_shapes=[
            pltpu.VMEM((count, 2, width, cols), jnp.bfloat16),
            pltpu.SemaphoreType.DMA((count, 2)),
        ],
        cost_estimate=pl.CostEstimate(
            flops=4 * rows * width * count * cols,
            bytes_accessed=2 * count * width * (rows + 2 * cols) + 4 * rows * cols,
            transcendentals=0,
        ),
        compiler_params=pltpu.CompilerParams(vmem_limit_bytes=16 << 20),
        name="project",
    )(*pieces, far(key_weight), far(value_weight))


def index_kernel(lines, plane, own_blocks, chosen_ref, slots_ref, *refs):
    asks = refs[: plane - 1]
    count, seen, rows = refs[plane - 1 :]
    size = own_blocks * TOPB
    device = lax.axis_index("kv")
    line = lax.div(device, plane)
    place = device - line * plane
    side_base = own_blocks * lines

    def clear(ref):
        def one(i, carry):
            ref[i] = 0
            return carry

        lax.fori_loop(0, ref.shape[0], one, 0)

    clear(count)
    clear(seen)
    clear(rows)

    def entry(e, carry):
        at = lax.div(e, TOPB)
        block = chosen_ref[at, e - at * TOPB]
        holder = lax.div(block, own_blocks)
        within = block - holder * own_blocks
        remote = holder != device
        spot = count[holder]
        count[holder] = spot + jnp.where(remote, 1, 0)
        spot = jnp.minimum(spot, CAP - 1)
        from_line = lax.div(holder, plane)
        from_place = holder - from_line * plane
        if plane & (plane - 1) == 0:
            shift = jnp.bitwise_xor(from_place, place)
        else:
            shift = lax.rem(from_place + place, plane)
        gap = jnp.maximum(line - from_line, 0)
        rows[(shift * lines + from_line) * CAP + spot] = within
        straight = gap * own_blocks + within
        across = side_base + (gap * (plane - 1) + shift - 1) * CAP + spot
        slots_ref[e] = jnp.where(from_place == place, straight, across)
        row = at + 1
        slots_ref[size + e] = jnp.where(seen[block] == row, 1, 0)
        seen[block] = row
        return carry

    lax.fori_loop(0, size, entry, 0)
    for shift, ask in enumerate(asks, 1):
        for i in range(lines * CAP):
            ask[i] = rows[shift * lines * CAP + i]


def index(chosen, lines, plane, own_blocks):
    size = own_blocks * TOPB
    ask = jax.ShapeDtypeStruct((lines * CAP,), jnp.int32)
    outs = pl.pallas_call(
        functools.partial(index_kernel, lines, plane, own_blocks),
        out_shape=[jax.ShapeDtypeStruct((2 * size,), jnp.int32)] + [ask] * (plane - 1),
        in_specs=[SMEM],
        out_specs=[SMEM] * plane,
        scratch_shapes=[
            pltpu.SMEM((lines * plane,), jnp.int32),
            pltpu.SMEM((lines * plane * own_blocks,), jnp.int32),
            pltpu.SMEM((plane * lines * CAP,), jnp.int32),
        ],
        compiler_params=pltpu.CompilerParams(vmem_limit_bytes=1 << 20),
        name="index",
    )(chosen)
    return outs[0], outs[1:]


def pick_kernel(targets, count, step, *refs):
    tables = refs[:targets]
    parts = refs[targets : targets + count]
    outs = refs[targets + count : -1]
    sems = refs[-1]
    line = lax.div(lax.axis_index("kv"), targets + 1)
    row = jnp.maximum(line - step, 0)
    copies = []
    for r, out in enumerate(outs):
        for i in range(CAP):
            block = tables[r][row * CAP + i]
            for t, part in enumerate(parts):
                cols = part.shape[2]
                copies.append(
                    pltpu.make_async_copy(
                        part.at[block],
                        out.at[i, :, pl.ds(t * cols, cols)],
                        sems.at[r, i, t],
                    )
                )
    for copy in copies:
        copy.start()
    for copy in copies:
        copy.wait()


def pick(tables, parts, step):
    targets = len(tables)
    _, rows, cols = parts[0].shape
    shape = jax.ShapeDtypeStruct((CAP, rows, cols * len(parts)), jnp.bfloat16)
    return pl.pallas_call(
        functools.partial(pick_kernel, targets, len(parts), step),
        out_shape=[shape] * targets,
        in_specs=[SMEM] * targets + [ANY] * len(parts),
        out_specs=[VMEM] * targets,
        scratch_shapes=[pltpu.SemaphoreType.DMA((targets, CAP, len(parts)))],
        compiler_params=pltpu.CompilerParams(vmem_limit_bytes=8 << 20),
        name="pick",
    )(*tables, *parts)


def attend_kernel(sizes, offsets, heads, group, first, *refs):
    n = len(sizes)
    slots_ref, q_ref = refs[:2]
    pool_refs = refs[2 : 2 + n]
    out_ref, pool, sems = refs[2 + n :]
    width = heads * HD
    copies = []
    at = 0
    for i, size in enumerate(sizes):
        part = pool_refs[i].at[:, :, pl.ds(offsets[i], 2 * width)]
        copies.append(
            pltpu.make_async_copy(part, pool.at[pl.ds(at, size)], sems.at[i])
        )
        at += size
    for copy in copies:
        copy.start()
    for copy in copies:
        copy.wait()
    blocks = q_ref.shape[0] // BLK
    low = lax.broadcasted_iota(jnp.int32, (1, 2 * BLK), 1) < BLK
    tri_row = lax.broadcasted_iota(jnp.int32, (BLK, HD), 0)
    tri_col = lax.broadcasted_iota(jnp.int32, (BLK, HD), 1)
    tri = jnp.where((tri_col < BLK) & (tri_col > tri_row), NEG, 0.0)
    tri = jnp.concatenate([tri] * group, axis=0)

    def block(b, carry):
        at_row = pl.multiple_of(b * BLK, BLK)
        picks = [slots_ref[b * TOPB + s] for s in range(TOPB)]
        hidden = [
            jnp.where(slots_ref[(blocks + b) * TOPB + s] > 0, NEG, 0.0)
            for s in range(TOPB)
        ]
        bias = jnp.concatenate(
            [jnp.where(low, hidden[s], hidden[s + 1]) for s in range(0, TOPB, 2)], axis=1
        )
        for j in range(heads):
            cols = [(j * group + g) * HD for g in range(group)]
            q = jnp.concatenate(
                [q_ref[pl.ds(at_row, BLK), first + c : first + c + HD] for c in cols],
                axis=0,
            )
            k = jnp.concatenate(
                [pool[p, :, j * HD : (j + 1) * HD] for p in picks], axis=0
            )
            v = jnp.concatenate(
                [pool[p, :, width + j * HD : width + (j + 1) * HD] for p in picks], axis=0
            )
            s = lax.dot_general(
                q, k, (((1,), (1,)), ((), ())), preferred_element_type=jnp.float32
            )
            s = s + bias
            s = jnp.concatenate([s[:, :HD] + tri, s[:, HD:]], axis=1)
            peak = jnp.max(s, axis=1, keepdims=True)
            w = jnp.exp((s - peak) * HD ** (-0.5))
            total = jnp.sum(w, axis=1, keepdims=True)
            o = jnp.dot(w.astype(jnp.bfloat16), v, preferred_element_type=jnp.float32)
            o = (o / total).astype(jnp.bfloat16)
            for g, c in enumerate(cols):
                out_ref[pl.ds(at_row, BLK), c : c + HD] = o[g * BLK : (g + 1) * BLK]
        return carry

    lax.fori_loop(0, blocks, block, 0)


def attend(queries, slots, pools, offsets, heads, group, first):
    rows = queries.shape[0]
    cols = heads * group * HD
    sizes = tuple(p.shape[0] for p in pools)
    return pl.pallas_call(
        functools.partial(attend_kernel, sizes, offsets, heads, group, first),
        out_shape=jax.ShapeDtypeStruct((rows, cols), jnp.bfloat16),
        in_specs=[SMEM, VMEM] + [ANY] * len(pools),
        out_specs=VMEM,
        scratch_shapes=[
            pltpu.VMEM((sum(sizes), BLK, 2 * heads * HD), jnp.bfloat16),
            pltpu.SemaphoreType.DMA((len(sizes),)),
        ],
        cost_estimate=pl.CostEstimate(
            flops=4 * rows * TOPB * BLK * cols,
            bytes_accessed=4 * rows * cols + 4 * sum(sizes) * BLK * heads * HD,
            transcendentals=rows * TOPB * BLK * cols // HD,
        ),
        compiler_params=pltpu.CompilerParams(vmem_limit_bytes=24 << 20),
        name="attend",
    )(slots, queries, *pools)


def local(tokens, query_weight, key_weight, value_weight, out_weight, chosen):
    tok_rows = tokens.shape[0]
    key_heads = key_weight.shape[1] // HD
    group = query_weight.shape[1] // HD // key_heads
    own_blocks = tok_rows // BLK
    devices = lax.axis_size("kv")
    plane = plane_size(devices)
    lines = devices // plane
    tp = lax.axis_size("tp")
    streams = 2 if key_heads % 2 == 0 else 1
    heads = key_heads // streams
    cols = heads * HD

    section = spread(tokens)
    up = [(d, (d + plane) % devices) for d in range(devices)]
    swaps = [
        [
            (l * plane + c, l * plane + partner(c, shift, plane))
            for l in range(lines)
            for c in range(plane)
        ]
        for shift in range(1, plane)
    ]

    own = []
    line_parts = [[] for _ in range(streams)]
    for t in range(streams):
        if t > 0:
            section, _ = lax.optimization_barrier((section, own[-1]))
        pair = project(section, key_weight, value_weight, t * cols, cols)
        own.append(pair.reshape(own_blocks, BLK, 2 * cols))
        if lines > 1:
            line_parts[t].append(send(own[t], up))
    chosen, _ = lax.optimization_barrier((chosen, own[-1]))
    slots, asks = index(chosen, lines, plane, own_blocks)
    asked = []
    for shift in range(1, plane):
        asked.append(send(asks[shift - 1], swaps[shift - 1]))

    side_parts = [[] for _ in range(streams)]
    offsets = [[] for _ in range(streams)]
    queries = None
    held = own
    for step in range(lines):
        last = step == lines - 1
        split = step >= lines - 2
        batches = [[t] for t in range(streams)] if split else [list(range(streams))]
        if last and queries is not None:
            held[0], queries = lax.optimization_barrier((held[0], queries))
        for batch in batches:
            if plane == 1:
                continue
            picked = pick(asked, [held[t] for t in batch], step)
            for shift in range(1, plane):
                got = send(picked[shift - 1], swaps[shift - 1])
                for i, t in enumerate(batch):
                    side_parts[t].append(got)
                    offsets[t].append(i * 2 * cols)
        if not last:
            held = [line_parts[t][-1] for t in range(streams)]
        if step + 1 < lines - 1:
            for t in range(streams):
                line_parts[t].append(send(held[t], up))
        if queries is None:
            queries = split_dot(section, query_weight)
    total = None
    me = lax.axis_index("tp")
    share = group * cols
    for t in range(streams):
        pools = [own[t]] + line_parts[t] + side_parts[t]
        shifts = (0,) * (1 + len(line_parts[t])) + tuple(offsets[t])
        done = attend(queries, slots, pools, shifts, heads, group, t * share)
        for shift, piece in enumerate(spread(done)):
            at = ((me + shift) % tp * streams + t) * share
            rows = lax.dynamic_slice_in_dim(out_weight, at, share, 0)
            term = jnp.dot(piece, rows, preferred_element_type=jnp.float32)
            total = term if total is None else total + term
    return total.astype(jnp.bfloat16)


def solution(mesh):
    return jax.shard_map(
        local,
        mesh=mesh,
        in_specs=(
            P("kv", "tp"),
            P(None, "tp"),
            P(None, "tp"),
            P(None, "tp"),
            P(None, "tp"),
            P("kv", None),
        ),
        out_specs=P("kv", "tp"),
        check_vma=False,
    )
```

```python
import functools
import math

import jax
import jax.numpy as jnp
from jax import lax
from jax.experimental import pallas as pl
from jax.experimental.pallas import tpu as pltpu
from jax.sharding import PartitionSpec as P


HD = 128
BLK = 64
TOPB = 16
CAP = 2
NEG = float("-inf")
VMEM = pl.BlockSpec(memory_space=pltpu.VMEM)
SMEM = pl.BlockSpec(memory_space=pltpu.SMEM)
ANY = pl.BlockSpec(memory_space=pl.ANY)


def plane_size(devices):
    return max(d for d in range(1, math.isqrt(devices) + 1) if devices % d == 0)


def partner(place, shift, plane):
    if plane & (plane - 1) == 0:
        return place ^ shift
    return (shift - place) % plane


def near(part):
    return pltpu.with_memory_space_constraint(part, pltpu.VMEM)


def far(part):
    return pltpu.with_memory_space_constraint(part, pltpu.HBM)


def send(part, pairs):
    return lax.ppermute(part, "kv", pairs)


def spread(part):
    count = lax.axis_size("tp")
    pieces = [part]
    for shift in range(1, count):
        pairs = [(i, (i - shift) % count) for i in range(count)]
        pieces.append(lax.ppermute(part, "tp", pairs))
    return pieces


def project_kernel(count, kinds, first, cols, *refs):
    pieces = refs[:count]
    weights = refs[count : count + kinds]
    out_ref, held, sems = refs[count + kinds :]
    width = pieces[0].shape[1]
    me = lax.axis_index("tp")
    copies = []
    for s in range(count):
        at = pl.multiple_of(lax.rem(me + s, count) * width, width)
        for i, ref in enumerate(weights):
            copy = pltpu.make_async_copy(
                ref.at[pl.ds(at, width), pl.ds(first, cols)],
                held.at[s, i],
                sems.at[s, i],
            )
            copy.start()
            copies.append(copy)
    totals = [None] * kinds
    for s in range(count):
        for i in range(kinds):
            copies[kinds * s + i].wait()
            term = jnp.dot(
                pieces[s][...], held[s, i], preferred_element_type=jnp.float32
            )
            totals[i] = term if s == 0 else totals[i] + term
    for i in range(kinds):
        out_ref[:, i * cols : (i + 1) * cols] = totals[i].astype(jnp.bfloat16)


def project(pieces, weights, first, cols):
    rows, width = pieces[0].shape
    count, kinds = len(pieces), len(weights)
    return pl.pallas_call(
        functools.partial(project_kernel, count, kinds, first, cols),
        out_shape=jax.ShapeDtypeStruct((rows, kinds * cols), jnp.bfloat16),
        in_specs=[VMEM] * count + [ANY] * kinds,
        out_specs=VMEM,
        scratch_shapes=[
            pltpu.VMEM((count, kinds, width, cols), jnp.bfloat16),
            pltpu.SemaphoreType.DMA((count, kinds)),
        ],
        cost_estimate=pl.CostEstimate(
            flops=2 * kinds * rows * width * count * cols,
            bytes_accessed=2 * count * width * (rows + kinds * cols),
            transcendentals=0,
        ),
        compiler_params=pltpu.CompilerParams(vmem_limit_bytes=16 << 20),
        name="project",
    )(*pieces, *[far(weight) for weight in weights])


def mix_kernel(streams, *refs):
    pieces = refs[:-2]
    weight_ref, out_ref = refs[-2:]
    count = len(pieces) // streams
    width = pieces[0].shape[1]
    step = min(2 * HD, out_ref.shape[1])
    me = lax.axis_index("tp")
    starts = [
        pl.multiple_of((lax.rem(me + s, count) * streams + t) * width, width)
        for t in range(streams)
        for s in range(count)
    ]
    for col in range(0, out_ref.shape[1], step):
        total = None
        for at, piece in zip(starts, pieces):
            rows = weight_ref[pl.ds(at, width), col : col + step]
            term = jnp.dot(piece[...], rows, preferred_element_type=jnp.float32)
            total = term if total is None else total + term
        out_ref[:, col : col + step] = total.astype(jnp.bfloat16)


def mix(pieces, weight, streams):
    rows, _ = pieces[0].shape
    depth, cols = weight.shape
    return pl.pallas_call(
        functools.partial(mix_kernel, streams),
        out_shape=jax.ShapeDtypeStruct((rows, cols), jnp.bfloat16),
        in_specs=[VMEM] * (len(pieces) + 1),
        out_specs=VMEM,
        cost_estimate=pl.CostEstimate(
            flops=2 * rows * depth * cols,
            bytes_accessed=2 * (rows * depth + depth * cols + rows * cols),
            transcendentals=0,
        ),
        compiler_params=pltpu.CompilerParams(vmem_limit_bytes=16 << 20),
        name="mix",
    )(*pieces, near(weight))


def index_kernel(lines, plane, own_blocks, chosen_ref, slots_ref, *refs):
    asks = refs[: plane - 1]
    count, seen, rows = refs[plane - 1 :]
    size = own_blocks * TOPB
    device = lax.axis_index("kv")
    line = lax.div(device, plane)
    place = device - line * plane
    side_base = own_blocks * lines

    def clear(ref):
        def one(i, carry):
            ref[i] = 0
            return carry

        lax.fori_loop(0, ref.shape[0], one, 0)

    clear(count)
    clear(seen)
    clear(rows)

    def entry(e, carry):
        at = lax.div(e, TOPB)
        block = chosen_ref[at, e - at * TOPB]
        holder = lax.div(block, own_blocks)
        within = block - holder * own_blocks
        remote = holder != device
        spot = count[holder]
        count[holder] = spot + jnp.where(remote, 1, 0)
        spot = jnp.minimum(spot, CAP - 1)
        from_line = lax.div(holder, plane)
        from_place = holder - from_line * plane
        if plane & (plane - 1) == 0:
            shift = jnp.bitwise_xor(from_place, place)
        else:
            shift = lax.rem(from_place + place, plane)
        gap = jnp.maximum(line - from_line, 0)
        rows[(shift * lines + from_line) * CAP + spot] = within
        straight = gap * own_blocks + within
        across = side_base + (gap * (plane - 1) + shift - 1) * CAP + spot
        slots_ref[e] = jnp.where(from_place == place, straight, across)
        row = at + 1
        slots_ref[size + e] = jnp.where(seen[block] == row, 1, 0)
        seen[block] = row
        return carry

    lax.fori_loop(0, size, entry, 0)
    for shift, ask in enumerate(asks, 1):
        for i in range(lines * CAP):
            ask[i] = rows[shift * lines * CAP + i]


def index(chosen, lines, plane, own_blocks):
    size = own_blocks * TOPB
    ask = jax.ShapeDtypeStruct((lines * CAP,), jnp.int32)
    outs = pl.pallas_call(
        functools.partial(index_kernel, lines, plane, own_blocks),
        out_shape=[jax.ShapeDtypeStruct((2 * size,), jnp.int32)] + [ask] * (plane - 1),
        in_specs=[SMEM],
        out_specs=[SMEM] * plane,
        scratch_shapes=[
            pltpu.SMEM((lines * plane,), jnp.int32),
            pltpu.SMEM((lines * plane * own_blocks,), jnp.int32),
            pltpu.SMEM((plane * lines * CAP,), jnp.int32),
        ],
        compiler_params=pltpu.CompilerParams(vmem_limit_bytes=1 << 20),
        name="index",
    )(chosen)
    return outs[0], outs[1:]


def pick_kernel(targets, count, step, *refs):
    tables = refs[:targets]
    parts = refs[targets : targets + count]
    outs = refs[targets + count : -1]
    sems = refs[-1]
    line = lax.div(lax.axis_index("kv"), targets + 1)
    row = jnp.maximum(line - step, 0)
    copies = []
    for r, out in enumerate(outs):
        for i in range(CAP):
            block = tables[r][row * CAP + i]
            for t, part in enumerate(parts):
                cols = part.shape[2]
                copies.append(
                    pltpu.make_async_copy(
                        part.at[block],
                        out.at[i, :, pl.ds(t * cols, cols)],
                        sems.at[r, i, t],
                    )
                )
    for copy in copies:
        copy.start()
    for copy in copies:
        copy.wait()


def pick(tables, parts, step):
    targets = len(tables)
    _, rows, cols = parts[0].shape
    shape = jax.ShapeDtypeStruct((CAP, rows, cols * len(parts)), jnp.bfloat16)
    return pl.pallas_call(
        functools.partial(pick_kernel, targets, len(parts), step),
        out_shape=[shape] * targets,
        in_specs=[SMEM] * targets + [ANY] * len(parts),
        out_specs=[VMEM] * targets,
        scratch_shapes=[pltpu.SemaphoreType.DMA((targets, CAP, len(parts)))],
        compiler_params=pltpu.CompilerParams(vmem_limit_bytes=8 << 20),
        name="pick",
    )(*tables, *parts)


def attend_kernel(sizes, offsets, heads, group, first, *refs):
    n = len(sizes)
    slots_ref, q_ref = refs[:2]
    pool_refs = refs[2 : 2 + n]
    out_ref, pool, sems = refs[2 + n :]
    width = heads * HD
    copies = []
    for j in range(heads):
        at = 0
        for i, size in enumerate(sizes):
            for kind in range(2):
                col = offsets[i] + kind * width + j * HD
                copies.append(
                    pltpu.make_async_copy(
                        pool_refs[i].at[:, :, pl.ds(col, HD)],
                        pool.at[j, kind, pl.ds(at, size)],
                        sems.at[j, kind, i],
                    )
                )
            at += size
    for copy in copies:
        copy.start()
    blocks = q_ref.shape[0] // BLK
    low = lax.broadcasted_iota(jnp.int32, (1, 2 * BLK), 1) < BLK
    tri_row = lax.broadcasted_iota(jnp.int32, (BLK, HD), 0)
    tri_col = lax.broadcasted_iota(jnp.int32, (BLK, HD), 1)
    tri = jnp.where((tri_col < BLK) & (tri_col > tri_row), NEG, 0.0)
    tri = jnp.concatenate([tri] * group, axis=0)
    ones = jnp.ones((TOPB * BLK, HD), jnp.bfloat16)

    def block(j, b, carry):
        at_row = pl.multiple_of(b * BLK, BLK)
        picks = [slots_ref[b * TOPB + s] for s in range(TOPB)]
        hidden = [
            jnp.where(slots_ref[(blocks + b) * TOPB + s] > 0, NEG, 0.0)
            for s in range(TOPB)
        ]
        bias = jnp.concatenate(
            [jnp.where(low, hidden[s], hidden[s + 1]) for s in range(0, TOPB, 2)], axis=1
        )
        cols = [(j * group + g) * HD for g in range(group)]
        q = jnp.concatenate(
            [q_ref[pl.ds(at_row, BLK), first + c : first + c + HD] for c in cols], axis=0
        )
        k = jnp.concatenate([pool[j, 0, p] for p in picks], axis=0)
        v = jnp.concatenate([pool[j, 1, p] for p in picks], axis=0)
        s = lax.dot_general(
            q, k, (((1,), (1,)), ((), ())), preferred_element_type=jnp.float32
        )
        s = s + bias
        s = jnp.concatenate([s[:, :HD] + tri, s[:, HD:]], axis=1)
        peak = jnp.max(s, axis=1, keepdims=True)
        w = jnp.exp2((s - peak) * (HD ** (-0.5) * math.log2(math.e)))
        v = jnp.concatenate([v, ones], axis=1)
        o = jnp.dot(w.astype(jnp.bfloat16), v, preferred_element_type=jnp.float32)
        o = (o[:, :HD] / o[:, HD:]).astype(jnp.bfloat16)
        for g, c in enumerate(cols):
            out_ref[pl.ds(at_row, BLK), c : c + HD] = o[g * BLK : (g + 1) * BLK]
        return carry

    each = 2 * n
    for j in range(heads):
        for copy in copies[j * each : (j + 1) * each]:
            copy.wait()
        lax.fori_loop(0, blocks, functools.partial(block, j), 0, unroll=blocks)


def attend(queries, slots, pools, offsets, heads, group, first):
    rows = queries.shape[0]
    cols = heads * group * HD
    sizes = tuple(p.shape[0] for p in pools)
    return pl.pallas_call(
        functools.partial(attend_kernel, sizes, offsets, heads, group, first),
        out_shape=jax.ShapeDtypeStruct((rows, cols), jnp.bfloat16),
        in_specs=[SMEM, VMEM] + [ANY] * len(pools),
        out_specs=VMEM,
        scratch_shapes=[
            pltpu.VMEM((heads, 2, sum(sizes), BLK, HD), jnp.bfloat16),
            pltpu.SemaphoreType.DMA((heads, 2, len(sizes))),
        ],
        cost_estimate=pl.CostEstimate(
            flops=4 * rows * TOPB * BLK * cols,
            bytes_accessed=4 * rows * cols + 4 * sum(sizes) * BLK * heads * HD,
            transcendentals=rows * TOPB * BLK * cols // HD,
        ),
        compiler_params=pltpu.CompilerParams(vmem_limit_bytes=12 << 20),
        name="attend",
    )(slots, queries, *pools)


def local(tokens, query_weight, key_weight, value_weight, out_weight, chosen):
    tok_rows = tokens.shape[0]
    key_heads = key_weight.shape[1] // HD
    group = query_weight.shape[1] // HD // key_heads
    own_blocks = tok_rows // BLK
    devices = lax.axis_size("kv")
    plane = plane_size(devices)
    lines = devices // plane
    streams = 2 if key_heads % 2 == 0 else 1
    heads = key_heads // streams
    cols = heads * HD

    section = spread(tokens)
    up = [(d, (d + plane) % devices) for d in range(devices)]
    swaps = [
        [
            (l * plane + c, l * plane + partner(c, shift, plane))
            for l in range(lines)
            for c in range(plane)
        ]
        for shift in range(1, plane)
    ]

    own = []
    line_parts = [[] for _ in range(streams)]
    for t in range(streams):
        if t > 0:
            section, _ = lax.optimization_barrier((section, own[-1]))
        pair = project(section, [key_weight, value_weight], t * cols, cols)
        own.append(pair.reshape(own_blocks, BLK, 2 * cols))
        if lines > 1:
            line_parts[t].append(send(own[t], up))
    chosen, _ = lax.optimization_barrier((chosen, own[-1]))
    slots, asks = index(chosen, lines, plane, own_blocks)
    asked = []
    for shift in range(1, plane):
        asked.append(send(asks[shift - 1], swaps[shift - 1]))

    side_parts = [[] for _ in range(streams)]
    offsets = [[] for _ in range(streams)]
    queries = None
    held = own
    for step in range(lines):
        last = step == lines - 1
        split = step >= lines - 2
        batches = [[t] for t in range(streams)] if split else [list(range(streams))]
        if last and queries is not None:
            held[0], queries = lax.optimization_barrier((held[0], queries))
        for batch in batches:
            if plane == 1:
                continue
            picked = pick(asked, [held[t] for t in batch], step)
            for shift in range(1, plane):
                got = send(picked[shift - 1], swaps[shift - 1])
                for i, t in enumerate(batch):
                    side_parts[t].append(got)
                    offsets[t].append(i * 2 * cols)
        if not last:
            held = [line_parts[t][-1] for t in range(streams)]
        if step + 1 < lines - 1:
            for t in range(streams):
                line_parts[t].append(send(held[t], up))
        if queries is None:
            queries = project(section, [query_weight], 0, query_weight.shape[1])
    share = group * cols
    done = []
    for t in range(streams):
        pools = [own[t]] + line_parts[t] + side_parts[t]
        shifts = (0,) * (1 + len(line_parts[t])) + tuple(offsets[t])
        done.append(attend(queries, slots, pools, shifts, heads, group, t * share))
    done = lax.optimization_barrier(done)
    pieces = [piece for part in done for piece in spread(part)]
    return mix(pieces, out_weight, streams)


def solution(mesh):
    return jax.shard_map(
        local,
        mesh=mesh,
        in_specs=(
            P("kv", "tp"),
            P(None, "tp"),
            P(None, "tp"),
            P(None, "tp"),
            P(None, "tp"),
            P("kv", None),
        ),
        out_specs=P("kv", "tp"),
        check_vma=False,
    )
```

```python
import functools
import math

import jax
import jax.numpy as jnp
from jax import lax
from jax.experimental import pallas as pl
from jax.experimental.pallas import tpu as pltpu
from jax.sharding import PartitionSpec as P


HD = 128
BLK = 64
TOPB = 16
CAP = 2
NEG = float("-inf")
VMEM = pl.BlockSpec(memory_space=pltpu.VMEM)
SMEM = pl.BlockSpec(memory_space=pltpu.SMEM)
ANY = pl.BlockSpec(memory_space=pl.ANY)


def plane_size(devices):
    return max(d for d in range(1, math.isqrt(devices) + 1) if devices % d == 0)


def partner(place, shift, plane):
    if plane & (plane - 1) == 0:
        return place ^ shift
    return (shift - place) % plane


def near(part):
    return pltpu.with_memory_space_constraint(part, pltpu.VMEM)


def far(part):
    return pltpu.with_memory_space_constraint(part, pltpu.HBM)


def send(part, pairs):
    return lax.ppermute(part, "kv", pairs)


def spread(part):
    count = lax.axis_size("tp")
    pieces = [part]
    for shift in range(1, count):
        pairs = [(i, (i - shift) % count) for i in range(count)]
        pieces.append(lax.ppermute(part, "tp", pairs))
    return pieces


def project_kernel(count, kinds, first, cols, *refs):
    pieces = refs[:count]
    weights = refs[count : count + kinds]
    out_ref, held, sems = refs[count + kinds :]
    width = pieces[0].shape[1]
    me = lax.axis_index("tp")
    copies = []
    for s in range(count):
        at = pl.multiple_of(lax.rem(me + s, count) * width, width)
        for i, ref in enumerate(weights):
            copy = pltpu.make_async_copy(
                ref.at[pl.ds(at, width), pl.ds(first, cols)],
                held.at[s, i],
                sems.at[s, i],
            )
            copy.start()
            copies.append(copy)
    totals = [None] * kinds
    for s in range(count):
        for i in range(kinds):
            copies[kinds * s + i].wait()
            term = jnp.dot(
                pieces[s][...], held[s, i], preferred_element_type=jnp.float32
            )
            totals[i] = term if s == 0 else totals[i] + term
    for i in range(kinds):
        out_ref[:, i * cols : (i + 1) * cols] = totals[i].astype(jnp.bfloat16)


def project(pieces, weights, first, cols):
    rows, width = pieces[0].shape
    count, kinds = len(pieces), len(weights)
    return pl.pallas_call(
        functools.partial(project_kernel, count, kinds, first, cols),
        out_shape=jax.ShapeDtypeStruct((rows, kinds * cols), jnp.bfloat16),
        in_specs=[VMEM] * count + [ANY] * kinds,
        out_specs=VMEM,
        scratch_shapes=[
            pltpu.VMEM((count, kinds, width, cols), jnp.bfloat16),
            pltpu.SemaphoreType.DMA((count, kinds)),
        ],
        cost_estimate=pl.CostEstimate(
            flops=2 * kinds * rows * width * count * cols,
            bytes_accessed=2 * count * width * (rows + kinds * cols),
            transcendentals=0,
        ),
        compiler_params=pltpu.CompilerParams(vmem_limit_bytes=16 << 20),
        name="project",
    )(*pieces, *[far(weight) for weight in weights])


def front_kernel(others, cols, own_in, key_ref, value_ref, own_ref, part_ref, rest_ref, held, sems):
    width = own_ref.shape[1]
    me = lax.axis_index("tp")
    own_copy = pltpu.make_async_copy(own_in, own_ref, sems.at[0, 0])
    own_copy.start()
    copies = []
    for s in range(others + 1):
        at = pl.multiple_of(lax.rem(me + s, others + 1) * width, width)
        for i, ref in enumerate((key_ref, value_ref)):
            target = held.at[i] if s == 0 else rest_ref.at[s - 1, i]
            copy = pltpu.make_async_copy(
                ref.at[pl.ds(at, width), pl.ds(0, cols)], target, sems.at[1 + s, i]
            )
            copy.start()
            copies.append(copy)
    own_copy.wait()
    for i in range(2):
        copies[i].wait()
        part_ref[:, i * cols : (i + 1) * cols] = jnp.dot(
            own_ref[...], held[i], preferred_element_type=jnp.float32
        )
    for copy in copies[2:]:
        copy.wait()


def front(own, key_weight, value_weight, cols):
    rows, width = own.shape
    others = lax.axis_size("tp") - 1
    return pl.pallas_call(
        functools.partial(front_kernel, others, cols),
        out_shape=[
            pltpu.VMEM((rows, width), jnp.bfloat16),
            pltpu.VMEM((rows, 2 * cols), jnp.float32),
            pltpu.VMEM((others, 2, width, cols), jnp.bfloat16),
        ],
        in_specs=[ANY] * 3,
        out_specs=[VMEM] * 3,
        scratch_shapes=[
            pltpu.VMEM((2, width, cols), jnp.bfloat16),
            pltpu.SemaphoreType.DMA((others + 2, 2)),
        ],
        compiler_params=pltpu.CompilerParams(vmem_limit_bytes=16 << 20),
        name="front",
    )(far(own), far(key_weight), far(value_weight))


def join_kernel(*refs):
    others = refs[:-3]
    part_ref, rest_ref, out_ref = refs[-3:]
    cols = rest_ref.shape[3]
    for i in range(2):
        span = slice(i * cols, (i + 1) * cols)
        total = part_ref[:, span]
        for s, other in enumerate(others):
            total = total + jnp.dot(
                other[...], rest_ref[s, i], preferred_element_type=jnp.float32
            )
        out_ref[:, span] = total.astype(jnp.bfloat16)


def join(others, part, rest):
    return pl.pallas_call(
        join_kernel,
        out_shape=jax.ShapeDtypeStruct(part.shape, jnp.bfloat16),
        in_specs=[VMEM] * (len(others) + 2),
        out_specs=VMEM,
        compiler_params=pltpu.CompilerParams(vmem_limit_bytes=16 << 20),
        name="join",
    )(*others, near(part), near(rest))


def mix_kernel(stream, streams, more, *refs):
    pieces = refs[: -2 - more]
    weight_ref, out_ref = refs[-2 - more], refs[-1]
    count = len(pieces)
    width = pieces[0].shape[1]
    step = min(2 * HD, out_ref.shape[1])
    me = lax.axis_index("tp")
    for col in range(0, out_ref.shape[1], step):
        span = slice(col, col + step)
        total = refs[-2][:, span] if more else None
        for s, piece in enumerate(pieces):
            at = pl.multiple_of((lax.rem(me + s, count) * streams + stream) * width, width)
            rows = weight_ref[pl.ds(at, width), span]
            term = jnp.dot(piece[...], rows, preferred_element_type=jnp.float32)
            total = term if total is None else total + term
        out_ref[:, span] = total.astype(out_ref.dtype)


def mix(pieces, weight, stream, streams, before):
    rows, width = pieces[0].shape
    cols = weight.shape[1]
    more = [] if before is None else [before]
    kind = jnp.bfloat16 if stream == streams - 1 else jnp.float32
    return pl.pallas_call(
        functools.partial(mix_kernel, stream, streams, len(more)),
        out_shape=jax.ShapeDtypeStruct((rows, cols), kind),
        in_specs=[VMEM] * (len(pieces) + 1 + len(more)),
        out_specs=VMEM,
        cost_estimate=pl.CostEstimate(
            flops=2 * rows * width * len(pieces) * cols,
            bytes_accessed=2 * width * len(pieces) * (rows + cols) + 4 * rows * cols,
            transcendentals=0,
        ),
        compiler_params=pltpu.CompilerParams(vmem_limit_bytes=16 << 20),
        name="mix",
    )(*pieces, near(weight), *more)


def quotient(value, divisor, limit):
    shift = 18
    factor = (1 << shift) // divisor + 1
    assert all(v * factor >> shift == v // divisor for v in range(limit))
    assert limit * factor < 1 << 31
    return lax.shift_right_logical(value * factor, shift)


def index_kernel(lines, plane, own_blocks, chosen_ref, slots_ref, *refs):
    asks = refs[: plane - 1]
    count, seen, rows = refs[plane - 1 :]
    size = own_blocks * TOPB
    devices = lines * plane
    device = lax.axis_index("kv")
    line = quotient(device, plane, devices)
    place = device - line * plane
    side_base = own_blocks * lines

    def clear(ref):
        def one(i, carry):
            ref[i] = 0
            return carry

        lax.fori_loop(0, ref.shape[0], one, 0, unroll=8)

    clear(count)
    clear(seen)
    clear(rows)

    def row(b, carry):
        for s in range(TOPB):
            e = b * TOPB + s
            block = chosen_ref[b, s]
            holder = quotient(block, own_blocks, devices * own_blocks)
            within = block - holder * own_blocks
            remote = holder != device
            spot = count[holder]
            count[holder] = spot + jnp.where(remote, 1, 0)
            spot = jnp.minimum(spot, CAP - 1)
            from_line = quotient(holder, plane, devices)
            from_place = holder - from_line * plane
            if plane & (plane - 1) == 0:
                shift = jnp.bitwise_xor(from_place, place)
            else:
                shift = lax.rem(from_place + place, plane)
            gap = jnp.maximum(line - from_line, 0)
            rows[(shift * lines + from_line) * CAP + spot] = within
            straight = gap * own_blocks + within
            across = side_base + (gap * (plane - 1) + shift - 1) * CAP + spot
            slots_ref[e] = jnp.where(from_place == place, straight, across)
            slots_ref[size + e] = jnp.where(seen[block] == b + 1, 1, 0)
            seen[block] = b + 1
        return carry

    lax.fori_loop(0, own_blocks, row, 0)
    for shift, ask in enumerate(asks, 1):
        for i in range(lines * CAP):
            ask[i] = rows[shift * lines * CAP + i]


def index(chosen, lines, plane, own_blocks):
    size = own_blocks * TOPB
    ask = jax.ShapeDtypeStruct((lines * CAP,), jnp.int32)
    outs = pl.pallas_call(
        functools.partial(index_kernel, lines, plane, own_blocks),
        out_shape=[jax.ShapeDtypeStruct((2 * size,), jnp.int32)] + [ask] * (plane - 1),
        in_specs=[SMEM],
        out_specs=[SMEM] * plane,
        scratch_shapes=[
            pltpu.SMEM((lines * plane,), jnp.int32),
            pltpu.SMEM((lines * plane * own_blocks,), jnp.int32),
            pltpu.SMEM((plane * lines * CAP,), jnp.int32),
        ],
        compiler_params=pltpu.CompilerParams(vmem_limit_bytes=1 << 20),
        name="index",
    )(chosen)
    return outs[0], outs[1:]


def pick_kernel(targets, count, step, *refs):
    tables = refs[:targets]
    parts = refs[targets : targets + count]
    outs = refs[targets + count : -1]
    sems = refs[-1]
    line = lax.div(lax.axis_index("kv"), targets + 1)
    row = jnp.maximum(line - step, 0)
    copies = []
    for r, out in enumerate(outs):
        for i in range(CAP):
            block = tables[r][row * CAP + i]
            for t, part in enumerate(parts):
                cols = part.shape[2]
                copies.append(
                    pltpu.make_async_copy(
                        part.at[block],
                        out.at[i, :, pl.ds(t * cols, cols)],
                        sems.at[r, i, t],
                    )
                )
    for copy in copies:
        copy.start()
    for copy in copies:
        copy.wait()


def pick(tables, parts, step):
    targets = len(tables)
    _, rows, cols = parts[0].shape
    shape = jax.ShapeDtypeStruct((CAP, rows, cols * len(parts)), jnp.bfloat16)
    return pl.pallas_call(
        functools.partial(pick_kernel, targets, len(parts), step),
        out_shape=[shape] * targets,
        in_specs=[SMEM] * targets + [ANY] * len(parts),
        out_specs=[VMEM] * targets,
        scratch_shapes=[pltpu.SemaphoreType.DMA((targets, CAP, len(parts)))],
        compiler_params=pltpu.CompilerParams(vmem_limit_bytes=8 << 20),
        name="pick",
    )(*tables, *parts)


def attend_kernel(sizes, offsets, heads, group, first, *refs):
    n = len(sizes)
    slots_ref, q_ref = refs[:2]
    pool_refs = refs[2 : 2 + n]
    out_ref, pool, sems = refs[2 + n :]
    width = heads * HD
    copies = []
    for j in range(heads):
        at = 0
        for i, size in enumerate(sizes):
            for kind in range(2):
                col = offsets[i] + kind * width + j * HD
                copies.append(
                    pltpu.make_async_copy(
                        pool_refs[i].at[:, :, pl.ds(col, HD)],
                        pool.at[j, kind, pl.ds(at, size)],
                        sems.at[j, kind, i],
                    )
                )
            at += size
    for copy in copies:
        copy.start()
    blocks = q_ref.shape[0] // BLK
    low = lax.broadcasted_iota(jnp.int32, (1, 2 * BLK), 1) < BLK
    tri_row = lax.broadcasted_iota(jnp.int32, (BLK, HD), 0)
    tri_col = lax.broadcasted_iota(jnp.int32, (BLK, HD), 1)
    tri = jnp.where((tri_col < BLK) & (tri_col > tri_row), NEG, 0.0)
    tri = jnp.concatenate([tri] * group, axis=0)
    ones = jnp.ones((TOPB * BLK, HD), jnp.bfloat16)

    def block(j, b, carry):
        at_row = pl.multiple_of(b * BLK, BLK)
        picks = [slots_ref[b * TOPB + s] for s in range(TOPB)]
        hidden = [
            jnp.where(slots_ref[(blocks + b) * TOPB + s] > 0, NEG, 0.0)
            for s in range(TOPB)
        ]
        bias = jnp.concatenate(
            [jnp.where(low, hidden[s], hidden[s + 1]) for s in range(0, TOPB, 2)], axis=1
        )
        cols = [(j * group + g) * HD for g in range(group)]
        q = jnp.concatenate(
            [q_ref[pl.ds(at_row, BLK), first + c : first + c + HD] for c in cols], axis=0
        )
        k = jnp.concatenate([pool[j, 0, p] for p in picks], axis=0)
        v = jnp.concatenate([pool[j, 1, p] for p in picks], axis=0)
        s = lax.dot_general(
            q, k, (((1,), (1,)), ((), ())), preferred_element_type=jnp.float32
        )
        s = s + bias
        s = jnp.concatenate([s[:, :HD] + tri, s[:, HD:]], axis=1)
        peak = jnp.max(s, axis=1, keepdims=True)
        w = jnp.exp2((s - peak) * (HD ** (-0.5) * math.log2(math.e)))
        v = jnp.concatenate([v, ones], axis=1)
        o = jnp.dot(w.astype(jnp.bfloat16), v, preferred_element_type=jnp.float32)
        o = (o[:, :HD] / o[:, HD:]).astype(jnp.bfloat16)
        for g, c in enumerate(cols):
            out_ref[pl.ds(at_row, BLK), c : c + HD] = o[g * BLK : (g + 1) * BLK]
        return carry

    each = 2 * n
    for j in range(heads):
        for copy in copies[j * each : (j + 1) * each]:
            copy.wait()
        lax.fori_loop(0, blocks, functools.partial(block, j), 0, unroll=blocks)


def attend(queries, slots, pools, offsets, heads, group, first):
    rows = queries.shape[0]
    cols = heads * group * HD
    sizes = tuple(p.shape[0] for p in pools)
    return pl.pallas_call(
        functools.partial(attend_kernel, sizes, offsets, heads, group, first),
        out_shape=jax.ShapeDtypeStruct((rows, cols), jnp.bfloat16),
        in_specs=[SMEM, VMEM] + [ANY] * len(pools),
        out_specs=VMEM,
        scratch_shapes=[
            pltpu.VMEM((heads, 2, sum(sizes), BLK, HD), jnp.bfloat16),
            pltpu.SemaphoreType.DMA((heads, 2, len(sizes))),
        ],
        cost_estimate=pl.CostEstimate(
            flops=4 * rows * TOPB * BLK * cols,
            bytes_accessed=4 * rows * cols + 4 * sum(sizes) * BLK * heads * HD,
            transcendentals=rows * TOPB * BLK * cols // HD,
        ),
        compiler_params=pltpu.CompilerParams(vmem_limit_bytes=12 << 20),
        name="attend",
    )(slots, queries, *pools)


def local(tokens, query_weight, key_weight, value_weight, out_weight, chosen):
    tok_rows = tokens.shape[0]
    key_heads = key_weight.shape[1] // HD
    group = query_weight.shape[1] // HD // key_heads
    own_blocks = tok_rows // BLK
    devices = lax.axis_size("kv")
    plane = plane_size(devices)
    lines = devices // plane
    streams = 2 if key_heads % 2 == 0 else 1
    heads = key_heads // streams
    cols = heads * HD

    tokens_here, part, rest = front(tokens, key_weight, value_weight, cols)
    section = [tokens_here] + spread(tokens)[1:]

    def up(hop):
        pairs = []
        for l in range(lines):
            to = l if l < hop else l + 1 if l < lines - 1 else hop
            pairs += [(l * plane + c, to * plane + c) for c in range(plane)]
        return pairs

    swaps = [
        [
            (l * plane + c, l * plane + partner(c, shift, plane))
            for l in range(lines)
            for c in range(plane)
        ]
        for shift in range(1, plane)
    ]

    own = []
    line_parts = [[] for _ in range(streams)]
    for t in range(streams):
        if t == 1:
            section, _ = lax.optimization_barrier((section, slots))
        if t == 0:
            pair = join(section[1:], part, rest)
        else:
            pair = project(section, [key_weight, value_weight], t * cols, cols)
        own.append(pair.reshape(own_blocks, BLK, 2 * cols))
        if lines > 1:
            line_parts[t].append(send(own[t], up(0)))
        if t == 0:
            chosen, _ = lax.optimization_barrier((chosen, own[0]))
            slots, asks = index(chosen, lines, plane, own_blocks)
    asked = []
    for shift in range(1, plane):
        asked.append(send(asks[shift - 1], swaps[shift - 1]))

    side_parts = [[] for _ in range(streams)]
    offsets = [[] for _ in range(streams)]
    queries = None
    held = own
    for step in range(lines):
        last = step == lines - 1
        split = step >= lines - 2
        batches = [[t] for t in range(streams)] if split else [list(range(streams))]
        if last and queries is not None:
            held[0], queries = lax.optimization_barrier((held[0], queries))
        for batch in batches:
            if plane == 1:
                continue
            picked = pick(asked, [held[t] for t in batch], step)
            for shift in range(1, plane):
                got = send(picked[shift - 1], swaps[shift - 1])
                for i, t in enumerate(batch):
                    side_parts[t].append(got)
                    offsets[t].append(i * 2 * cols)
        if not last:
            held = [line_parts[t][-1] for t in range(streams)]
        if step + 1 < lines - 1:
            for t in range(streams):
                line_parts[t].append(send(held[t], up(step + 1)))
        if queries is None:
            queries = project(section, [query_weight], 0, query_weight.shape[1])
    share = group * cols
    total = None
    for t in range(streams):
        pools = [own[t]] + line_parts[t] + side_parts[t]
        shifts = (0,) * (1 + len(line_parts[t])) + tuple(offsets[t])
        done = attend(queries, slots, pools, shifts, heads, group, t * share)
        total = mix(spread(done), out_weight, t, streams, total)
    return total


def solution(mesh):
    return jax.shard_map(
        local,
        mesh=mesh,
        in_specs=(
            P("kv", "tp"),
            P(None, "tp"),
            P(None, "tp"),
            P(None, "tp"),
            P(None, "tp"),
            P("kv", None),
        ),
        out_specs=P("kv", "tp"),
        check_vma=False,
    )
```

```python
import functools
import math

import jax
import jax.numpy as jnp
from jax import lax
from jax.experimental import pallas as pl
from jax.experimental.pallas import tpu as pltpu
from jax.sharding import PartitionSpec as P


HD = 128
BLK = 64
TOPB = 16
CAP = 2
NEG = float("-inf")
VMEM = pl.BlockSpec(memory_space=pltpu.VMEM)
SMEM = pl.BlockSpec(memory_space=pltpu.SMEM)
ANY = pl.BlockSpec(memory_space=pl.ANY)


def plane_size(devices):
    return max(d for d in range(1, math.isqrt(devices) + 1) if devices % d == 0)


def partner(place, shift, plane):
    if plane & (plane - 1) == 0:
        return place ^ shift
    return (shift - place) % plane


def near(part):
    return pltpu.with_memory_space_constraint(part, pltpu.VMEM)


def far(part):
    return pltpu.with_memory_space_constraint(part, pltpu.HBM)


def send(part, pairs):
    return lax.ppermute(part, "kv", pairs)


def spread(part):
    count = lax.axis_size("tp")
    pieces = [part]
    for shift in range(1, count):
        pairs = [(i, (i - shift) % count) for i in range(count)]
        pieces.append(lax.ppermute(part, "tp", pairs))
    return pieces


def project_kernel(count, kinds, first, cols, *refs):
    pieces = refs[:count]
    weights = refs[count : count + kinds]
    out_ref, held, sems = refs[count + kinds :]
    width = pieces[0].shape[1]
    me = lax.axis_index("tp")
    copies = []
    for s in range(count):
        at = pl.multiple_of(lax.rem(me + s, count) * width, width)
        for i, ref in enumerate(weights):
            copy = pltpu.make_async_copy(
                ref.at[pl.ds(at, width), pl.ds(first, cols)],
                held.at[s, i],
                sems.at[s, i],
            )
            copy.start()
            copies.append(copy)
    totals = [None] * kinds
    for s in range(count):
        for i in range(kinds):
            copies[kinds * s + i].wait()
            term = jnp.dot(
                pieces[s][...], held[s, i], preferred_element_type=jnp.float32
            )
            totals[i] = term if s == 0 else totals[i] + term
    for i in range(kinds):
        out_ref[:, i * cols : (i + 1) * cols] = totals[i].astype(jnp.bfloat16)


def project(pieces, weights, first, cols):
    rows, width = pieces[0].shape
    count, kinds = len(pieces), len(weights)
    return pl.pallas_call(
        functools.partial(project_kernel, count, kinds, first, cols),
        out_shape=jax.ShapeDtypeStruct((rows, kinds * cols), jnp.bfloat16),
        in_specs=[VMEM] * count + [ANY] * kinds,
        out_specs=VMEM,
        scratch_shapes=[
            pltpu.VMEM((count, kinds, width, cols), jnp.bfloat16),
            pltpu.SemaphoreType.DMA((count, kinds)),
        ],
        cost_estimate=pl.CostEstimate(
            flops=2 * kinds * rows * width * count * cols,
            bytes_accessed=2 * count * width * (rows + kinds * cols),
            transcendentals=0,
        ),
        compiler_params=pltpu.CompilerParams(vmem_limit_bytes=16 << 20),
        name="project",
    )(*pieces, *[far(weight) for weight in weights])


def front_kernel(others, cols, own_in, key_ref, value_ref, own_ref, part_ref, rest_ref, held, sems):
    width = own_ref.shape[1]
    me = lax.axis_index("tp")
    own_copy = pltpu.make_async_copy(own_in, own_ref, sems.at[0, 0])
    own_copy.start()
    copies = []
    for s in range(others + 1):
        at = pl.multiple_of(lax.rem(me + s, others + 1) * width, width)
        for i, ref in enumerate((key_ref, value_ref)):
            target = held.at[i] if s == 0 else rest_ref.at[s - 1, i]
            copy = pltpu.make_async_copy(
                ref.at[pl.ds(at, width), pl.ds(0, cols)], target, sems.at[1 + s, i]
            )
            copy.start()
            copies.append(copy)
    own_copy.wait()
    for i in range(2):
        copies[i].wait()
        part_ref[:, i * cols : (i + 1) * cols] = jnp.dot(
            own_ref[...], held[i], preferred_element_type=jnp.float32
        )
    for copy in copies[2:]:
        copy.wait()


def front(own, key_weight, value_weight, cols):
    rows, width = own.shape
    others = lax.axis_size("tp") - 1
    return pl.pallas_call(
        functools.partial(front_kernel, others, cols),
        out_shape=[
            pltpu.VMEM((rows, width), jnp.bfloat16),
            pltpu.VMEM((rows, 2 * cols), jnp.float32),
            pltpu.VMEM((others, 2, width, cols), jnp.bfloat16),
        ],
        in_specs=[ANY] * 3,
        out_specs=[VMEM] * 3,
        scratch_shapes=[
            pltpu.VMEM((2, width, cols), jnp.bfloat16),
            pltpu.SemaphoreType.DMA((others + 2, 2)),
        ],
        compiler_params=pltpu.CompilerParams(vmem_limit_bytes=16 << 20),
        name="front",
    )(far(own), far(key_weight), far(value_weight))


def join_kernel(*refs):
    others = refs[:-3]
    part_ref, rest_ref, out_ref = refs[-3:]
    cols = rest_ref.shape[3]
    for i in range(2):
        span = slice(i * cols, (i + 1) * cols)
        total = part_ref[:, span]
        for s, other in enumerate(others):
            total = total + jnp.dot(
                other[...], rest_ref[s, i], preferred_element_type=jnp.float32
            )
        out_ref[:, span] = total.astype(jnp.bfloat16)


def join(others, part, rest):
    return pl.pallas_call(
        join_kernel,
        out_shape=jax.ShapeDtypeStruct(part.shape, jnp.bfloat16),
        in_specs=[VMEM] * (len(others) + 2),
        out_specs=VMEM,
        compiler_params=pltpu.CompilerParams(vmem_limit_bytes=16 << 20),
        name="join",
    )(*others, near(part), near(rest))


def mix_kernel(part, streams, more, *refs):
    pieces = refs[: -2 - more]
    weight_ref, out_ref = refs[-2 - more], refs[-1]
    count = lax.axis_size("tp")
    width = pieces[0].shape[1]
    step = min(2 * HD, out_ref.shape[1])
    me = lax.axis_index("tp")
    starts = [
        pl.multiple_of((lax.rem(me + s, count) * streams + t) * width, width)
        for t, s in part
    ]
    for col in range(0, out_ref.shape[1], step):
        span = slice(col, col + step)
        total = refs[-2][:, span] if more else None
        for at, piece in zip(starts, pieces):
            rows = weight_ref[pl.ds(at, width), span]
            term = jnp.dot(piece[...], rows, preferred_element_type=jnp.float32)
            total = term if total is None else total + term
        out_ref[:, span] = total.astype(out_ref.dtype)


def mix(pieces, part, weight, streams, before, last):
    rows, width = pieces[0].shape
    cols = weight.shape[1]
    more = [] if before is None else [before]
    return pl.pallas_call(
        functools.partial(mix_kernel, part, streams, len(more)),
        out_shape=jax.ShapeDtypeStruct((rows, cols), jnp.bfloat16 if last else jnp.float32),
        in_specs=[VMEM] * (len(pieces) + 1 + len(more)),
        out_specs=VMEM,
        cost_estimate=pl.CostEstimate(
            flops=2 * rows * width * len(pieces) * cols,
            bytes_accessed=2 * width * len(pieces) * (rows + cols) + 4 * rows * cols,
            transcendentals=0,
        ),
        compiler_params=pltpu.CompilerParams(vmem_limit_bytes=16 << 20),
        name="mix",
    )(*pieces, near(weight), *more)


def quotient(value, divisor, limit):
    shift = 18
    factor = (1 << shift) // divisor + 1
    assert all(v * factor >> shift == v // divisor for v in range(limit))
    assert limit * factor < 1 << 31
    return lax.shift_right_logical(value * factor, shift)


def index_kernel(lines, plane, own_blocks, chosen_ref, slots_ref, *refs):
    asks = refs[: plane - 1]
    count, seen, rows = refs[plane - 1 :]
    size = own_blocks * TOPB
    devices = lines * plane
    device = lax.axis_index("kv")
    line = quotient(device, plane, devices)
    place = device - line * plane
    side_base = own_blocks * lines

    def clear(ref):
        def one(i, carry):
            ref[i] = 0
            return carry

        lax.fori_loop(0, ref.shape[0], one, 0, unroll=8)

    clear(count)
    clear(seen)
    clear(rows)

    def row(b, carry):
        for s in range(TOPB):
            e = b * TOPB + s
            block = chosen_ref[b, s]
            holder = quotient(block, own_blocks, devices * own_blocks)
            within = block - holder * own_blocks
            remote = holder != device
            spot = count[holder]
            count[holder] = spot + jnp.where(remote, 1, 0)
            spot = jnp.minimum(spot, CAP - 1)
            from_line = quotient(holder, plane, devices)
            from_place = holder - from_line * plane
            if plane & (plane - 1) == 0:
                shift = jnp.bitwise_xor(from_place, place)
            else:
                shift = lax.rem(from_place + place, plane)
            gap = jnp.maximum(line - from_line, 0)
            rows[(shift * lines + from_line) * CAP + spot] = within
            straight = gap * own_blocks + within
            across = side_base + (gap * (plane - 1) + shift - 1) * CAP + spot
            slots_ref[e] = jnp.where(from_place == place, straight, across)
            slots_ref[size + e] = jnp.where(seen[block] == b + 1, 1, 0)
            seen[block] = b + 1
        return carry

    lax.fori_loop(0, own_blocks, row, 0)
    for shift, ask in enumerate(asks, 1):
        for i in range(lines * CAP):
            ask[i] = rows[shift * lines * CAP + i]


def index(chosen, lines, plane, own_blocks):
    size = own_blocks * TOPB
    ask = jax.ShapeDtypeStruct((lines * CAP,), jnp.int32)
    outs = pl.pallas_call(
        functools.partial(index_kernel, lines, plane, own_blocks),
        out_shape=[jax.ShapeDtypeStruct((2 * size,), jnp.int32)] + [ask] * (plane - 1),
        in_specs=[SMEM],
        out_specs=[SMEM] * plane,
        scratch_shapes=[
            pltpu.SMEM((lines * plane,), jnp.int32),
            pltpu.SMEM((lines * plane * own_blocks,), jnp.int32),
            pltpu.SMEM((plane * lines * CAP,), jnp.int32),
        ],
        compiler_params=pltpu.CompilerParams(vmem_limit_bytes=1 << 20),
        name="index",
    )(chosen)
    return outs[0], outs[1:]


def pick_kernel(targets, count, step, *refs):
    tables = refs[:targets]
    parts = refs[targets : targets + count]
    outs = refs[targets + count :]
    line = lax.div(lax.axis_index("kv"), targets + 1)
    row = jnp.maximum(line - step, 0)
    for table, out in zip(tables, outs):
        for i in range(CAP):
            block = table[row * CAP + i]
            for t, part in enumerate(parts):
                cols = part.shape[2]
                out[i, :, t * cols : (t + 1) * cols] = part[block]


def pick(tables, parts, step):
    targets = len(tables)
    _, rows, cols = parts[0].shape
    shape = pltpu.VMEM((CAP, rows, cols * len(parts)), jnp.bfloat16)
    return pl.pallas_call(
        functools.partial(pick_kernel, targets, len(parts), step),
        out_shape=[shape] * targets,
        in_specs=[SMEM] * targets + [VMEM] * len(parts),
        out_specs=[VMEM] * targets,
        compiler_params=pltpu.CompilerParams(vmem_limit_bytes=8 << 20),
        name="pick",
    )(*tables, *[near(part) for part in parts])


def attend_kernel(offsets, heads, group, first, *refs):
    slots_ref, q_ref = refs[:2]
    parts = refs[2:-2]
    out_ref, pool = refs[-2:]
    at = 0
    for part, offset in zip(parts, offsets):
        for j in range(heads):
            for kind in range(2):
                col = offset + (kind * heads + j) * HD
                pool[j, kind, at : at + part.shape[0]] = part[:, :, col : col + HD]
        at += part.shape[0]
    blocks = q_ref.shape[0] // BLK
    low = lax.broadcasted_iota(jnp.int32, (1, 2 * BLK), 1) < BLK
    tri_row = lax.broadcasted_iota(jnp.int32, (BLK, HD), 0)
    tri_col = lax.broadcasted_iota(jnp.int32, (BLK, HD), 1)
    tri = jnp.where((tri_col < BLK) & (tri_col > tri_row), NEG, 0.0)
    tri = jnp.concatenate([tri] * group, axis=0)
    ones = jnp.ones((TOPB * BLK, HD), jnp.bfloat16)

    def block(j, b, carry):
        at_row = pl.multiple_of(b * BLK, BLK)
        picks = [slots_ref[b * TOPB + s] for s in range(TOPB)]
        hidden = [
            jnp.where(slots_ref[(blocks + b) * TOPB + s] > 0, NEG, 0.0)
            for s in range(TOPB)
        ]
        bias = jnp.concatenate(
            [jnp.where(low, hidden[s], hidden[s + 1]) for s in range(0, TOPB, 2)], axis=1
        )
        cols = [(j * group + g) * HD for g in range(group)]
        q = jnp.concatenate(
            [q_ref[pl.ds(at_row, BLK), first + c : first + c + HD] for c in cols], axis=0
        )
        k = jnp.concatenate([pool[j, 0, p] for p in picks], axis=0)
        v = jnp.concatenate([pool[j, 1, p] for p in picks], axis=0)
        s = lax.dot_general(
            q, k, (((1,), (1,)), ((), ())), preferred_element_type=jnp.float32
        )
        s = s + bias
        s = jnp.concatenate([s[:, :HD] + tri, s[:, HD:]], axis=1)
        peak = jnp.max(s, axis=1, keepdims=True)
        w = jnp.exp2((s - peak) * (HD ** (-0.5) * math.log2(math.e)))
        v = jnp.concatenate([v, ones], axis=1)
        o = jnp.dot(w.astype(jnp.bfloat16), v, preferred_element_type=jnp.float32)
        o = (o[:, :HD] / o[:, HD:]).astype(jnp.bfloat16)
        for g, c in enumerate(cols):
            out_ref[pl.ds(at_row, BLK), c : c + HD] = o[g * BLK : (g + 1) * BLK]
        return carry

    for j in range(heads):
        lax.fori_loop(0, blocks, functools.partial(block, j), 0, unroll=blocks)


def attend(queries, slots, parts, offsets, heads, group, first):
    rows = queries.shape[0]
    cols = heads * group * HD
    size = sum(part.shape[0] for part in parts)
    return pl.pallas_call(
        functools.partial(attend_kernel, offsets, heads, group, first),
        out_shape=jax.ShapeDtypeStruct((rows, cols), jnp.bfloat16),
        in_specs=[SMEM, VMEM] + [VMEM] * len(parts),
        out_specs=VMEM,
        scratch_shapes=[pltpu.VMEM((heads, 2, size, BLK, HD), jnp.bfloat16)],
        cost_estimate=pl.CostEstimate(
            flops=4 * rows * TOPB * BLK * cols,
            bytes_accessed=4 * rows * cols + 4 * size * BLK * heads * HD,
            transcendentals=rows * TOPB * BLK * cols // HD,
        ),
        compiler_params=pltpu.CompilerParams(vmem_limit_bytes=12 << 20),
        name="attend",
    )(slots, queries, *[near(part) for part in parts])


def local(tokens, query_weight, key_weight, value_weight, out_weight, chosen):
    tok_rows = tokens.shape[0]
    key_heads = key_weight.shape[1] // HD
    group = query_weight.shape[1] // HD // key_heads
    own_blocks = tok_rows // BLK
    devices = lax.axis_size("kv")
    plane = plane_size(devices)
    lines = devices // plane
    tp = lax.axis_size("tp")
    streams = 2 if key_heads % 2 == 0 else 1
    heads = key_heads // streams
    cols = heads * HD

    tokens_here, part, rest = front(tokens, key_weight, value_weight, cols)
    section = [tokens_here] + spread(tokens)[1:]

    def up(hop):
        pairs = []
        for l in range(lines):
            to = l if l < hop else l + 1 if l < lines - 1 else hop
            pairs += [(l * plane + c, to * plane + c) for c in range(plane)]
        return pairs

    swaps = [
        [
            (l * plane + c, l * plane + partner(c, shift, plane))
            for l in range(lines)
            for c in range(plane)
        ]
        for shift in range(1, plane)
    ]

    own = []
    line_parts = [[] for _ in range(streams)]
    for t in range(streams):
        if t == 1:
            section, _ = lax.optimization_barrier((section, slots))
        if t == 0:
            pair = join(section[1:], part, rest)
        else:
            pair = project(section, [key_weight, value_weight], t * cols, cols)
        own.append(pair.reshape(own_blocks, BLK, 2 * cols))
        if lines > 1:
            line_parts[t].append(send(own[t], up(0)))
        if t == 0:
            chosen, _ = lax.optimization_barrier((chosen, own[0]))
            slots, asks = index(chosen, lines, plane, own_blocks)
    asked = []
    for shift in range(1, plane):
        asked.append(send(asks[shift - 1], swaps[shift - 1]))

    side_parts = [[] for _ in range(streams)]
    offsets = [[] for _ in range(streams)]
    queries = None
    held = own
    for step in range(lines):
        last = step == lines - 1
        split = step >= lines - 2
        batches = [[t] for t in range(streams)] if split else [list(range(streams))]
        if last and queries is not None:
            held[0], queries = lax.optimization_barrier((held[0], queries))
        for batch in batches:
            if plane == 1:
                continue
            picked = pick(asked, [held[t] for t in batch], step)
            for shift in range(1, plane):
                got = send(picked[shift - 1], swaps[shift - 1])
                for i, t in enumerate(batch):
                    side_parts[t].append(got)
                    offsets[t].append(i * 2 * cols)
        if not last:
            held = [line_parts[t][-1] for t in range(streams)]
        if step + 1 < lines - 1:
            for t in range(streams):
                line_parts[t].append(send(held[t], up(step + 1)))
        if queries is None:
            queries = project(section, [query_weight], 0, query_weight.shape[1])
    share = group * cols
    pieces = []
    for t in range(streams):
        parts = [own[t]] + line_parts[t] + side_parts[t]
        shifts = [0] * (1 + len(line_parts[t])) + offsets[t]
        done = attend(queries, slots, parts, shifts, heads, group, t * share)
        pieces.append(spread(done))
    early = [(t, s) for t in range(streams) for s in range(tp)][: streams * tp - tp + 1]
    rest = [(streams - 1, s) for s in range(1, tp)]
    total = None
    for part in (early, rest):
        if part:
            total = mix(
                [pieces[t][s] for t, s in part], part, out_weight, streams, total, part == rest
            )
    return total


def solution(mesh):
    return jax.shard_map(
        local,
        mesh=mesh,
        in_specs=(
            P("kv", "tp"),
            P(None, "tp"),
            P(None, "tp"),
            P(None, "tp"),
            P(None, "tp"),
            P("kv", None),
        ),
        out_specs=P("kv", "tp"),
        check_vma=False,
    )
```

```python
import functools
import math

import jax
import jax.numpy as jnp
from jax import lax
from jax.experimental import pallas as pl
from jax.experimental.pallas import tpu as pltpu
from jax.sharding import PartitionSpec as P


HD = 128
BLK = 64
TOPB = 16
CAP = 2
NEG = float("-inf")
VMEM = pl.BlockSpec(memory_space=pltpu.VMEM)
SMEM = pl.BlockSpec(memory_space=pltpu.SMEM)
ANY = pl.BlockSpec(memory_space=pl.ANY)


def plane_size(devices):
    return max(d for d in range(1, math.isqrt(devices) + 1) if devices % d == 0)


def partner(place, shift, plane):
    if plane & (plane - 1) == 0:
        return place ^ shift
    return (shift - place) % plane


def near(part):
    return pltpu.with_memory_space_constraint(part, pltpu.VMEM)


def far(part):
    return pltpu.with_memory_space_constraint(part, pltpu.HBM)


def send(part, pairs):
    return lax.ppermute(part, "kv", pairs)


def spread(part):
    count = lax.axis_size("tp")
    pieces = [part]
    for shift in range(1, count):
        pairs = [(i, (i - shift) % count) for i in range(count)]
        pieces.append(lax.ppermute(part, "tp", pairs))
    return pieces


def project_kernel(count, kinds, first, cols, *refs):
    pieces = refs[:count]
    weights = refs[count : count + kinds]
    out_ref, held, sems = refs[count + kinds :]
    width = pieces[0].shape[1]
    me = lax.axis_index("tp")
    copies = []
    for s in range(count):
        at = pl.multiple_of(lax.rem(me + s, count) * width, width)
        for i, ref in enumerate(weights):
            copy = pltpu.make_async_copy(
                ref.at[pl.ds(at, width), pl.ds(first, cols)],
                held.at[s, i],
                sems.at[s, i],
            )
            copy.start()
            copies.append(copy)
    totals = [None] * kinds
    for s in range(count):
        for i in range(kinds):
            copies[kinds * s + i].wait()
            term = jnp.dot(
                pieces[s][...], held[s, i], preferred_element_type=jnp.float32
            )
            totals[i] = term if s == 0 else totals[i] + term
    for i in range(kinds):
        out_ref[:, i * cols : (i + 1) * cols] = totals[i].astype(jnp.bfloat16)


def project(pieces, weights, first, cols):
    rows, width = pieces[0].shape
    count, kinds = len(pieces), len(weights)
    return pl.pallas_call(
        functools.partial(project_kernel, count, kinds, first, cols),
        out_shape=jax.ShapeDtypeStruct((rows, kinds * cols), jnp.bfloat16),
        in_specs=[VMEM] * count + [ANY] * kinds,
        out_specs=VMEM,
        scratch_shapes=[
            pltpu.VMEM((count, kinds, width, cols), jnp.bfloat16),
            pltpu.SemaphoreType.DMA((count, kinds)),
        ],
        cost_estimate=pl.CostEstimate(
            flops=2 * kinds * rows * width * count * cols,
            bytes_accessed=2 * count * width * (rows + kinds * cols),
            transcendentals=0,
        ),
        compiler_params=pltpu.CompilerParams(vmem_limit_bytes=16 << 20),
        name="project",
    )(*pieces, *[far(weight) for weight in weights])


def front_kernel(others, cols, own_in, key_ref, value_ref, own_ref, part_ref, rest_ref, held, sems):
    width = own_ref.shape[1]
    me = lax.axis_index("tp")
    own_copy = pltpu.make_async_copy(own_in, own_ref, sems.at[0, 0])
    own_copy.start()
    copies = []
    for s in range(others + 1):
        at = pl.multiple_of(lax.rem(me + s, others + 1) * width, width)
        for i, ref in enumerate((key_ref, value_ref)):
            target = held.at[i] if s == 0 else rest_ref.at[s - 1, i]
            copy = pltpu.make_async_copy(
                ref.at[pl.ds(at, width), pl.ds(0, cols)], target, sems.at[1 + s, i]
            )
            copy.start()
            copies.append(copy)
    own_copy.wait()
    for i in range(2):
        copies[i].wait()
        part_ref[:, i * cols : (i + 1) * cols] = jnp.dot(
            own_ref[...], held[i], preferred_element_type=jnp.float32
        )
    for copy in copies[2:]:
        copy.wait()


def front(own, key_weight, value_weight, cols):
    rows, width = own.shape
    others = lax.axis_size("tp") - 1
    return pl.pallas_call(
        functools.partial(front_kernel, others, cols),
        out_shape=[
            pltpu.VMEM((rows, width), jnp.bfloat16),
            pltpu.VMEM((rows, 2 * cols), jnp.float32),
            pltpu.VMEM((others, 2, width, cols), jnp.bfloat16),
        ],
        in_specs=[ANY] * 3,
        out_specs=[VMEM] * 3,
        scratch_shapes=[
            pltpu.VMEM((2, width, cols), jnp.bfloat16),
            pltpu.SemaphoreType.DMA((others + 2, 2)),
        ],
        compiler_params=pltpu.CompilerParams(vmem_limit_bytes=16 << 20),
        name="front",
    )(far(own), far(key_weight), far(value_weight))


def join_kernel(*refs):
    others = refs[:-3]
    part_ref, rest_ref, out_ref = refs[-3:]
    cols = rest_ref.shape[3]
    for i in range(2):
        span = slice(i * cols, (i + 1) * cols)
        total = part_ref[:, span]
        for s, other in enumerate(others):
            total = total + jnp.dot(
                other[...], rest_ref[s, i], preferred_element_type=jnp.float32
            )
        out_ref[:, span] = total.astype(jnp.bfloat16)


def join(others, part, rest):
    return pl.pallas_call(
        join_kernel,
        out_shape=jax.ShapeDtypeStruct(part.shape, jnp.bfloat16),
        in_specs=[VMEM] * (len(others) + 2),
        out_specs=VMEM,
        compiler_params=pltpu.CompilerParams(vmem_limit_bytes=16 << 20),
        name="join",
    )(*others, near(part), near(rest))


def mix_kernel(part, streams, more, last, *refs):
    home = refs[-3] if last else None
    out_ref, sems = refs[-2:] if last else (refs[-1], None)
    refs = refs[:-3] if last else refs[:-1]
    pieces = refs[: -1 - more]
    weight_ref = refs[-1 - more]
    count = lax.axis_size("tp")
    width = pieces[0].shape[1]
    step = min(2 * HD, out_ref.shape[1])
    me = lax.axis_index("tp")
    starts = [
        pl.multiple_of((lax.rem(me + s, count) * streams + t) * width, width)
        for t, s in part
    ]
    copies = []
    for i, col in enumerate(range(0, out_ref.shape[1], step)):
        span = slice(col, col + step)
        total = refs[-1][:, span] if more else None
        for at, piece in zip(starts, pieces):
            rows = weight_ref[pl.ds(at, width), span]
            term = jnp.dot(piece[...], rows, preferred_element_type=jnp.float32)
            total = term if total is None else total + term
        out_ref[:, span] = total.astype(out_ref.dtype)
        if last:
            copy = pltpu.make_async_copy(out_ref.at[:, span], home.at[:, span], sems.at[i])
            copy.start()
            copies.append(copy)
    for copy in copies:
        copy.wait()


def mix(pieces, part, weight, streams, before, last):
    rows, width = pieces[0].shape
    cols = weight.shape[1]
    more = [] if before is None else [before]
    return pl.pallas_call(
        functools.partial(mix_kernel, part, streams, len(more), last),
        out_shape=jax.ShapeDtypeStruct((rows, cols), jnp.bfloat16 if last else jnp.float32),
        in_specs=[VMEM] * (len(pieces) + 1 + len(more)),
        out_specs=ANY if last else VMEM,
        scratch_shapes=[
            pltpu.VMEM((rows, cols), jnp.bfloat16),
            pltpu.SemaphoreType.DMA((pl.cdiv(cols, 2 * HD),)),
        ]
        if last
        else [],
        cost_estimate=pl.CostEstimate(
            flops=2 * rows * width * len(pieces) * cols,
            bytes_accessed=2 * width * len(pieces) * (rows + cols) + 4 * rows * cols,
            transcendentals=0,
        ),
        compiler_params=pltpu.CompilerParams(vmem_limit_bytes=16 << 20),
        name="mix",
    )(*pieces, near(weight), *more)


def quotient(value, divisor, limit):
    shift = 18
    factor = (1 << shift) // divisor + 1
    assert all(v * factor >> shift == v // divisor for v in range(limit))
    assert limit * factor < 1 << 31
    return lax.shift_right_logical(value * factor, shift)


def index_kernel(lines, plane, own_blocks, chosen_ref, slots_ref, *refs):
    asks = refs[: plane - 1]
    count, seen, rows = refs[plane - 1 :]
    size = own_blocks * TOPB
    devices = lines * plane
    device = lax.axis_index("kv")
    line = quotient(device, plane, devices)
    place = device - line * plane
    side_base = own_blocks * lines

    def clear(ref):
        def one(i, carry):
            ref[i] = 0
            return carry

        lax.fori_loop(0, ref.shape[0], one, 0, unroll=8)

    clear(count)
    clear(seen)
    clear(rows)

    def row(b, carry):
        for s in range(TOPB):
            e = b * TOPB + s
            block = chosen_ref[b, s]
            holder = quotient(block, own_blocks, devices * own_blocks)
            within = block - holder * own_blocks
            remote = holder != device
            spot = count[holder]
            count[holder] = spot + jnp.where(remote, 1, 0)
            spot = jnp.minimum(spot, CAP - 1)
            from_line = quotient(holder, plane, devices)
            from_place = holder - from_line * plane
            if plane & (plane - 1) == 0:
                shift = jnp.bitwise_xor(from_place, place)
            else:
                shift = lax.rem(from_place + place, plane)
            gap = jnp.maximum(line - from_line, 0)
            rows[(shift * lines + from_line) * CAP + spot] = within
            straight = gap * own_blocks + within
            across = side_base + (gap * (plane - 1) + shift - 1) * CAP + spot
            slots_ref[e] = jnp.where(from_place == place, straight, across)
            slots_ref[size + e] = jnp.where(seen[block] == b + 1, 1, 0)
            seen[block] = b + 1
        return carry

    lax.fori_loop(0, own_blocks, row, 0)
    for shift, ask in enumerate(asks, 1):
        for i in range(lines * CAP):
            ask[i] = rows[shift * lines * CAP + i]


def index(chosen, lines, plane, own_blocks):
    size = own_blocks * TOPB
    ask = jax.ShapeDtypeStruct((lines * CAP,), jnp.int32)
    outs = pl.pallas_call(
        functools.partial(index_kernel, lines, plane, own_blocks),
        out_shape=[jax.ShapeDtypeStruct((2 * size,), jnp.int32)] + [ask] * (plane - 1),
        in_specs=[SMEM],
        out_specs=[SMEM] * plane,
        scratch_shapes=[
            pltpu.SMEM((lines * plane,), jnp.int32),
            pltpu.SMEM((lines * plane * own_blocks,), jnp.int32),
            pltpu.SMEM((plane * lines * CAP,), jnp.int32),
        ],
        compiler_params=pltpu.CompilerParams(vmem_limit_bytes=1 << 20),
        name="index",
    )(chosen)
    return outs[0], outs[1:]


def pick_kernel(targets, count, step, *refs):
    tables = refs[:targets]
    parts = refs[targets : targets + count]
    outs = refs[targets + count :]
    line = lax.div(lax.axis_index("kv"), targets + 1)
    row = jnp.maximum(line - step, 0)
    for table, out in zip(tables, outs):
        for i in range(CAP):
            block = table[row * CAP + i]
            for t, part in enumerate(parts):
                cols = part.shape[2]
                out[i, :, t * cols : (t + 1) * cols] = part[block]


def pick(tables, parts, step):
    targets = len(tables)
    _, rows, cols = parts[0].shape
    shape = pltpu.VMEM((CAP, rows, cols * len(parts)), jnp.bfloat16)
    return pl.pallas_call(
        functools.partial(pick_kernel, targets, len(parts), step),
        out_shape=[shape] * targets,
        in_specs=[SMEM] * targets + [VMEM] * len(parts),
        out_specs=[VMEM] * targets,
        compiler_params=pltpu.CompilerParams(vmem_limit_bytes=8 << 20),
        name="pick",
    )(*tables, *[near(part) for part in parts])


def attend_kernel(offsets, heads, group, first, *refs):
    slots_ref, q_ref = refs[:2]
    parts = refs[2:-2]
    out_ref, pool = refs[-2:]
    at = 0
    for part, offset in zip(parts, offsets):
        for j in range(heads):
            for kind in range(2):
                col = offset + (kind * heads + j) * HD
                pool[j, kind, at : at + part.shape[0]] = part[:, :, col : col + HD]
        at += part.shape[0]
    blocks = q_ref.shape[0] // BLK
    low = lax.broadcasted_iota(jnp.int32, (1, 2 * BLK), 1) < BLK
    tri_row = lax.broadcasted_iota(jnp.int32, (BLK, HD), 0)
    tri_col = lax.broadcasted_iota(jnp.int32, (BLK, HD), 1)
    tri = jnp.where((tri_col < BLK) & (tri_col > tri_row), NEG, 0.0)
    tri = jnp.concatenate([tri] * group, axis=0)
    ones = jnp.ones((TOPB * BLK, HD), jnp.bfloat16)

    def block(j, b, carry):
        at_row = pl.multiple_of(b * BLK, BLK)
        picks = [slots_ref[b * TOPB + s] for s in range(TOPB)]
        hidden = [
            jnp.where(slots_ref[(blocks + b) * TOPB + s] > 0, NEG, 0.0)
            for s in range(TOPB)
        ]
        bias = jnp.concatenate(
            [jnp.where(low, hidden[s], hidden[s + 1]) for s in range(0, TOPB, 2)], axis=1
        )
        cols = [(j * group + g) * HD for g in range(group)]
        q = jnp.concatenate(
            [q_ref[pl.ds(at_row, BLK), first + c : first + c + HD] for c in cols], axis=0
        )
        k = jnp.concatenate([pool[j, 0, p] for p in picks], axis=0)
        v = jnp.concatenate([pool[j, 1, p] for p in picks], axis=0)
        s = lax.dot_general(
            q, k, (((1,), (1,)), ((), ())), preferred_element_type=jnp.float32
        )
        s = s + bias
        s = jnp.concatenate([s[:, :HD] + tri, s[:, HD:]], axis=1)
        peak = jnp.max(s, axis=1, keepdims=True)
        w = jnp.exp2((s - peak) * (HD ** (-0.5) * math.log2(math.e)))
        v = jnp.concatenate([v, ones], axis=1)
        o = jnp.dot(w.astype(jnp.bfloat16), v, preferred_element_type=jnp.float32)
        o = (o[:, :HD] / o[:, HD:]).astype(jnp.bfloat16)
        for g, c in enumerate(cols):
            out_ref[pl.ds(at_row, BLK), c : c + HD] = o[g * BLK : (g + 1) * BLK]
        return carry

    for j in range(heads):
        lax.fori_loop(0, blocks, functools.partial(block, j), 0, unroll=blocks)


def attend(queries, slots, parts, offsets, heads, group, first):
    rows = queries.shape[0]
    cols = heads * group * HD
    size = sum(part.shape[0] for part in parts)
    return pl.pallas_call(
        functools.partial(attend_kernel, offsets, heads, group, first),
        out_shape=jax.ShapeDtypeStruct((rows, cols), jnp.bfloat16),
        in_specs=[SMEM, VMEM] + [VMEM] * len(parts),
        out_specs=VMEM,
        scratch_shapes=[pltpu.VMEM((heads, 2, size, BLK, HD), jnp.bfloat16)],
        cost_estimate=pl.CostEstimate(
            flops=4 * rows * TOPB * BLK * cols,
            bytes_accessed=4 * rows * cols + 4 * size * BLK * heads * HD,
            transcendentals=rows * TOPB * BLK * cols // HD,
        ),
        compiler_params=pltpu.CompilerParams(vmem_limit_bytes=12 << 20),
        name="attend",
    )(slots, queries, *[near(part) for part in parts])


def local(tokens, query_weight, key_weight, value_weight, out_weight, chosen):
    tok_rows = tokens.shape[0]
    key_heads = key_weight.shape[1] // HD
    group = query_weight.shape[1] // HD // key_heads
    own_blocks = tok_rows // BLK
    devices = lax.axis_size("kv")
    plane = plane_size(devices)
    lines = devices // plane
    tp = lax.axis_size("tp")
    streams = 2 if key_heads % 2 == 0 else 1
    heads = key_heads // streams
    cols = heads * HD

    tokens_here, part, rest = front(tokens, key_weight, value_weight, cols)
    section = [tokens_here] + spread(tokens)[1:]

    def up(hop):
        pairs = []
        for l in range(lines):
            to = l if l < hop else l + 1 if l < lines - 1 else hop
            pairs += [(l * plane + c, to * plane + c) for c in range(plane)]
        return pairs

    swaps = [
        [
            (l * plane + c, l * plane + partner(c, shift, plane))
            for l in range(lines)
            for c in range(plane)
        ]
        for shift in range(1, plane)
    ]

    own = []
    line_parts = [[] for _ in range(streams)]
    for t in range(streams):
        if t == 1:
            section, _ = lax.optimization_barrier((section, slots))
        if t == 0:
            pair = join(section[1:], part, rest)
        else:
            pair = project(section, [key_weight, value_weight], t * cols, cols)
        own.append(pair.reshape(own_blocks, BLK, 2 * cols))
        if lines > 1:
            line_parts[t].append(send(own[t], up(0)))
        if t == 0:
            chosen, _ = lax.optimization_barrier((chosen, own[0]))
            slots, asks = index(chosen, lines, plane, own_blocks)
    asked = []
    for shift in range(1, plane):
        asked.append(send(asks[shift - 1], swaps[shift - 1]))

    side_parts = [[] for _ in range(streams)]
    offsets = [[] for _ in range(streams)]
    queries = None
    held = own
    for step in range(lines):
        last = step == lines - 1
        split = step >= 1
        batches = [[t] for t in range(streams)] if split else [list(range(streams))]
        if last and queries is not None:
            held[0], queries = lax.optimization_barrier((held[0], queries))
        for batch in batches:
            if plane == 1:
                continue
            picked = pick(asked, [held[t] for t in batch], step)
            for shift in range(1, plane):
                got = send(picked[shift - 1], swaps[shift - 1])
                for i, t in enumerate(batch):
                    side_parts[t].append(got)
                    offsets[t].append(i * 2 * cols)
        if not last:
            held = [line_parts[t][-1] for t in range(streams)]
        if step + 1 < lines - 1:
            for t in range(streams):
                line_parts[t].append(send(held[t], up(step + 1)))
        if queries is None:
            queries = project(section, [query_weight], 0, query_weight.shape[1])
    share = group * cols
    pieces = []
    for t in range(streams):
        parts = [own[t]] + line_parts[t] + side_parts[t]
        shifts = [0] * (1 + len(line_parts[t])) + offsets[t]
        done = attend(queries, slots, parts, shifts, heads, group, t * share)
        pieces.append(spread(done))
    early = [(t, s) for t in range(streams) for s in range(tp)][: streams * tp - tp + 1]
    rest = [(streams - 1, s) for s in range(1, tp)]
    total = None
    for part in (early, rest):
        if part:
            total = mix(
                [pieces[t][s] for t, s in part], part, out_weight, streams, total, part == rest
            )
    return total


def solution(mesh):
    return jax.shard_map(
        local,
        mesh=mesh,
        in_specs=(
            P("kv", "tp"),
            P(None, "tp"),
            P(None, "tp"),
            P(None, "tp"),
            P(None, "tp"),
            P("kv", None),
        ),
        out_specs=P("kv", "tp"),
        check_vma=False,
    )
```
